32 devices in a mesh: fs: 8 (over z, x), tp: 4 (over y, core).
Axes of the slice: x: 2, y: 2, z: 4, core: 2. Of those that a mesh axis runs over, the one named last changes fastest.
Arguments:
- tokens: bfloat16 [1024, 2048], P('fs', 'tp'), may hold values from -6 to 6
- routes: int32 [1024, 2], P('fs'), may hold values from 0 to 3, all different within a row; in each aligned block of 128 rows (0 to 127, 128 to 255, ...) at most 96 rows name the same one
- route_weight: float32 [1024, 2], P('fs'), may hold values from 0.1 to 1
- norm_gain: float32 [2048], P('fs'), may hold values from 0.1 to 1.9
- expert_gate: float32 [4, 2048, 512], P(None, 'fs', 'tp'), may hold values from -0.125 to 0.125
- expert_up: float32 [4, 2048, 512], P(None, 'fs', 'tp'), may hold values from -0.125 to 0.125
- expert_down: float32 [4, 2048, 512], P(None, 'fs', 'tp'), may hold values from -0.25 to 0.25
- shared_gate: float32 [2048, 512], P('fs', 'tp'), may hold values from -0.125 to 0.125
- shared_up: float32 [2048, 512], P('fs', 'tp'), may hold values from -0.125 to 0.125
- shared_down: float32 [512, 2048], P('tp', 'fs'), may hold values from -0.25 to 0.25
Outputs:
- mixed: bfloat16 [1024, 2048], P('fs', 'tp')
- gate_sampler: bfloat16 [8, 2048, 256], P('fs', None, 'tp')
- up_sampler: bfloat16 [8, 2048, 256], P('fs', None, 'tp')
- down_sampler: bfloat16 [8, 2048, 256], P('fs', 'tp')
- shared_gate_out: bfloat16 [2048, 512], P(None, 'tp')
- shared_up_out: bfloat16 [2048, 512], P(None, 'tp')
- shared_down_out: bfloat16 [512, 2048], P('tp')
The draws below stay inside these ranges and needn't reach their ends.
Inputs may be any that keep to these rules, and one draw needn't show every extreme that they name: `routes`: each row names 2 different experts. In each aligned block of 128 rows no expert is named by more than 96 rows, a bound that some block reaches.
All inputs are finite; a program needn't handle non-finite values.
Results may differ from the reference program's by a relative error of at most 0.009.
Values may be sent and summed in bfloat16 or wider, within the bound.
A program may use at most 64 MiB of HBM per device.

```python
import math
import jax
import jax.numpy as jnp
import numpy as np
from jax import lax

D = 2048
FF = 512
TOP_K = 2
TOK_DEV = 128
EXPERTS = 4
UNITS = 64
SHARED_BLOCK = 128
CAP = 96
TOKENS = 1024
N_FS = 8
N_TP = 4


def steps_of(rng, shape, split, least, high):
    gain = 1.0
    for dim, blocks in split:
        heights = jax.random.uniform(jax.random.fold_in(jax.random.fold_in(rng, 6), dim), (blocks,), jnp.float32, least / len(split), high / len(split))
        gain = gain * jnp.repeat(jnp.exp(heights), shape[dim] // blocks).reshape((-1,) + (1,) * (len(shape) - 1 - dim))
    return gain


def routed_block(own_key, own, number, rows, number_of, top, most, slope):
    sequence = jax.random.permutation(own_key, number_of)
    heavy_load, ordinary = shares(number_of, rows * top, most, slope, True), shares(number_of, rows * top, most, slope, False)
    places = jnp.arange(number_of)

    def named(sizes, turn):
        used = int((sizes > 0).sum())
        fixed = max(1, used // 4)
        passed = fixed + (places - fixed + turn * (used - fixed)) % max(1, number_of - fixed)
        return jnp.zeros((number_of,), jnp.int32).at[sequence[jnp.where(places < fixed, places, passed)]].set(jnp.asarray(sizes, jnp.int32))

    sizes = jnp.where(number % 4 == 0, named(heavy_load, number // 4), named(ordinary, number - number // 4 - 1))
    mixed = jax.random.permutation(jax.random.fold_in(own, 3), number_of)
    giver, sink = mixed[0:number_of // 2 * 2:2], mixed[1:number_of // 2 * 2:2]
    margin = jnp.minimum(sizes[giver] - 1, most - sizes[sink]) // 2
    margin = jnp.where((giver == sequence[0]) | (sink == sequence[0]) | (sizes[sink] == 0), 0, jnp.maximum(margin, 0))
    passed = jax.random.randint(jax.random.fold_in(own, 4), (number_of // 2,), 0, 1 << 20) % (margin + 1)
    sizes = sizes.at[giver].add(-passed).at[sink].add(passed)
    items = jnp.searchsorted(jnp.cumsum(sizes), jnp.arange(rows * top), side="right").astype(jnp.int32)
    table = items.reshape(top, rows).T
    table = table[jax.random.permutation(jax.random.fold_in(own, 1), rows)]
    turn = jax.random.randint(jax.random.fold_in(own, 2), (rows, 1), 0, top)
    return jnp.take_along_axis(table, (jnp.arange(top)[None, :] + turn) % top, axis=1)


def shares(amount, total, limit, lean, full):
    portions = [(1 << 20) // math.isqrt(rank ** lean) + 1 for rank in range(1, amount + 1)]
    largest = limit if full else min(limit, max(-(-total // amount), total * portions[0] // sum(portions)))
    least = 1 if total - largest >= amount - 1 else 0
    given, rest = [largest] + [least] * (amount - 1), total - largest - least * (amount - 1)
    while rest > 0:
        movable = [i for i in range(1, amount) if given[i] < largest] or [i for i in range(1, amount) if given[i] < limit]
        mass, budget = sum([portions[i] for i in movable]), rest
        for i in movable:
            addition = min(limit - given[i], max(1, budget * portions[i] // mass), rest)
            given[i] = given[i] + addition
            rest = rest - addition
    return np.array(given)


def noise(stream_key, extent, width, bound, pieces=(), held_as=jnp.bfloat16):
    gain = steps_of(stream_key, extent, pieces, -0.22, 0.18) if pieces else 1.0
    values = jax.random.normal(stream_key, extent, jnp.float32) * width * gain
    return jnp.minimum(jnp.maximum(values, -bound), bound).astype(held_as)


def setup_inputs(seed: int = 0) -> dict:
    keys = jax.random.split(jax.random.key(seed), 11)
    tokens = noise(keys[0], (TOKENS, D), 1.0, 6.0, ((0, 8), (1, 4)))
    routes_keys = jax.random.split(jax.random.fold_in(keys[1], 1), TOKENS // TOK_DEV)
    routes_turns = jax.random.permutation(jax.random.fold_in(keys[1], 3), TOKENS // TOK_DEV)
    routes = jax.vmap(lambda own, number: routed_block(jax.random.fold_in(keys[1], 2), own, number, TOK_DEV, EXPERTS, TOP_K, CAP, 0))(routes_keys, routes_turns).reshape((TOKENS, TOP_K))
    route_weight = jnp.clip(0.1 + 0.9 * jax.random.uniform(keys[2], (TOKENS, TOP_K), jnp.float32) ** steps_of(keys[2], (TOKENS, TOP_K), ((0, 8),), -0.2, 0.2), 0.1, 1.0)
    norm_gain = jnp.clip(1.0 + 0.18 * jax.random.normal(keys[3], (D,), jnp.float32), 0.1, 1.9)
    expert_gate = noise(keys[4], (EXPERTS, D, FF), D ** -0.5, 0.125, ((1, 8), (2, 4)), jnp.float32)
    expert_up = noise(keys[5], (EXPERTS, D, FF), D ** -0.5, 0.125, ((1, 8), (2, 4)), jnp.float32)
    expert_down = noise(keys[6], (EXPERTS, D, FF), FF ** -0.5, 0.25, ((1, 8), (2, 4)), jnp.float32)
    shared_gate = noise(keys[7], (D, FF), D ** -0.5, 0.125, ((0, 8), (1, 4)), jnp.float32)
    shared_up = noise(keys[8], (D, FF), D ** -0.5, 0.125, ((0, 8), (1, 4)), jnp.float32)
    shared_down = noise(keys[9], (FF, D), FF ** -0.5, 0.25, ((0, 4), (1, 8)), jnp.float32)
    return {"tokens": tokens, "routes": routes, "route_weight": route_weight, "norm_gain": norm_gain, "expert_gate": expert_gate, "expert_up": expert_up, "expert_down": expert_down, "shared_gate": shared_gate, "shared_up": shared_up, "shared_down": shared_down}


EPS = 1e-06

def slot_places(routes):
    blocks = routes.reshape(N_FS, TOK_DEV * TOP_K)
    onehot = (blocks[:, :, None] == jnp.arange(EXPERTS, dtype=jnp.int32)[None, None, :]).astype(jnp.int32)
    earlier = jnp.cumsum(onehot, axis=1) - onehot
    position = lax.optimization_barrier(jnp.sum(earlier * onehot, axis=2))
    return (blocks * CAP + position).astype(jnp.int32)

def to_sampler(folded):
    return folded.reshape(EXPERTS, D, N_TP, 2, UNITS).transpose(0, 3, 1, 2, 4).reshape(2 * EXPERTS, D, N_TP * UNITS)

def reference(tokens, routes, route_weight, norm_gain, expert_gate, expert_up, expert_down, shared_gate, shared_up, shared_down):
    gate_folded = (expert_gate * norm_gain[None, :, None]).astype(jnp.bfloat16)
    up_folded = (expert_up * norm_gain[None, :, None]).astype(jnp.bfloat16)
    down_round = expert_down.astype(jnp.bfloat16)
    gate_sampler = to_sampler(gate_folded)
    up_sampler = to_sampler(up_folded)
    down_sampler = to_sampler(down_round)
    shared_gate_out = (shared_gate * norm_gain[:, None]).astype(jnp.bfloat16)
    shared_up_out = (shared_up * norm_gain[:, None]).astype(jnp.bfloat16)
    shared_down_out = shared_down.astype(jnp.bfloat16)
    tokens_wide = tokens.astype(jnp.float32)
    normed = (tokens_wide * lax.rsqrt(lax.optimization_barrier(jnp.mean(tokens_wide * tokens_wide, axis=1, keepdims=True)) + EPS)).astype(jnp.bfloat16)
    shared_act = jnp.dot(normed, shared_gate_out, preferred_element_type=jnp.float32)
    shared_lin = jnp.dot(normed, shared_up_out, preferred_element_type=jnp.float32)
    shared_hidden = (jax.nn.silu(shared_act) * shared_lin).astype(jnp.bfloat16)
    shared_sum = jnp.zeros((TOKENS, D), jnp.float32)
    for tp_part in range(N_TP):
        lower = tp_part * SHARED_BLOCK
        product = jnp.dot(shared_hidden[:, lower:lower + SHARED_BLOCK], shared_down_out[lower:lower + SHARED_BLOCK], preferred_element_type=jnp.float32)
        shared_sum = shared_sum + lax.optimization_barrier(product.astype(jnp.bfloat16)).astype(jnp.float32)
    places = slot_places(routes)
    block_ids = jnp.arange(N_FS, dtype=jnp.int32)[:, None]
    token_ids = (block_ids * TOK_DEV + jnp.arange(TOK_DEV * TOP_K, dtype=jnp.int32)[None, :] // TOP_K).astype(jnp.int32)
    slot_table = jnp.full((N_FS, EXPERTS * CAP), TOKENS, jnp.int32).at[block_ids, places].set(token_ids)
    slot_weight = jnp.zeros((N_FS, EXPERTS * CAP), jnp.float32).at[block_ids, places].set(route_weight.reshape(N_FS, TOK_DEV * TOP_K))
    slot_table = slot_table.reshape(N_FS, EXPERTS, CAP).transpose(1, 0, 2).reshape(EXPERTS, N_FS * CAP)
    slot_weight = slot_weight.reshape(N_FS, EXPERTS, CAP).transpose(1, 0, 2).reshape(EXPERTS, N_FS * CAP)
    padded = jnp.concatenate([normed, jnp.zeros((1, D), jnp.bfloat16)], axis=0)

    def expert_step(totals, inputs):
        row_ids, weights, gate_rows, up_rows, down_rows = inputs
        picked = padded[row_ids]
        gate_act = jnp.dot(picked, gate_rows, preferred_element_type=jnp.float32)
        up_act = jnp.dot(picked, up_rows, preferred_element_type=jnp.float32)
        hidden = (jax.nn.silu(gate_act) * up_act).astype(jnp.bfloat16).reshape(N_FS * CAP, N_TP, 2, UNITS)
        down_parts = down_rows.reshape(D, N_TP, 2, UNITS)
        combined = jnp.zeros((N_FS * CAP, D), jnp.float32)
        for half_index in range(2):
            down_half = down_parts[:, :, half_index, :].reshape(D, N_TP * UNITS)
            product = jnp.dot(hidden[:, :, half_index, :].reshape(N_FS * CAP, N_TP * UNITS), down_half.T, preferred_element_type=jnp.float32)
            combined = combined + lax.optimization_barrier(product.astype(jnp.bfloat16)).astype(jnp.float32)
        return (totals.at[row_ids].add(combined * weights[:, None]), None)
    routed_total, _ = lax.scan(expert_step, jnp.zeros((TOKENS + 1, D), jnp.float32), (slot_table, slot_weight, gate_folded, up_folded, down_round))
    mixed = (shared_sum + routed_total[:TOKENS]).astype(jnp.bfloat16)
    return (mixed, gate_sampler, up_sampler, down_sampler, shared_gate_out, shared_up_out, shared_down_out)
```

```python
import functools

import jax
import jax.numpy as jnp
from jax import lax
from jax.experimental import pallas as pl
from jax.experimental.pallas import tpu as pltpu
from jax.sharding import PartitionSpec as P

EPS = 1e-06
BF = jnp.bfloat16
F32 = jnp.float32


def loop(low, high, body):
    def step(i, carry):
        body(i)
        return carry

    lax.fori_loop(low, high, step, 0)


def dot(a, b):
    return jnp.dot(a, b, preferred_element_type=F32)


def dot_nt(a, b):
    return lax.dot_general(a, b, (((1,), (1,)), ((), ())), preferred_element_type=F32)


def left_halves(a, b, half):
    lane = lax.broadcasted_iota(jnp.int32, a.shape, 1)
    return jnp.where(lane < half, a, pltpu.roll(b, half, 1))


def right_halves(a, b, half):
    lane = lax.broadcasted_iota(jnp.int32, a.shape, 1)
    return jnp.where(lane < half, pltpu.roll(a, half, 1), b)


def silu(v):
    return v / (1.0 + jnp.exp(-v))


def kernel(
    F,
    T,
    slots,
    tok_in,
    routes_in,
    weight_in,
    gain_in,
    eg_in,
    eu_in,
    ed_in,
    sg_in,
    su_in,
    sd_in,
    mixed,
    gate_out,
    up_out,
    dn_out,
    sg_out,
    su_out,
    sd_out,
    tok,
    routes,
    weight,
    gain,
    eg,
    eu,
    ed,
    sg,
    su,
    sd,
    s_load,
    tk,
    nm,
    gu_send,
    gu,
    dn_send,
    dn,
    sh,
    disp,
    port,
    hid,
    away,
    keep,
    near,
    ret_send,
    ret,
    part,
    shr,
    s_tok,
    r_tok,
    s_gu,
    r_gu,
    s_dn,
    r_dn,
    s_left,
    s_right,
    s_shb,
    r_sh,
    s_da,
    s_db,
    s_out,
    s_in,
    r_port,
    s_hid,
    r_hid,
    s_near,
    r_near,
    s_ret,
    r_ret,
    s_shr,
    r_shr,
):
    G = F // 2
    K = F // T
    E = eg.shape[0]
    R, C = eg.shape[1], eg.shape[2]
    half = C // 2
    tok_count = tok.shape[0]
    quarter = tok.shape[1]
    width = quarter * T
    f = lax.axis_index("fs")
    t = lax.axis_index("tp")
    g, p = f // 2, f % 2
    pair = g * 2 + (1 - p)
    t_pair = (t // 2) * 2 + (1 - t % 2)

    def remote(src, dst, send, recv, fs, tp):
        return pltpu.make_async_remote_copy(
            src_ref=src,
            dst_ref=dst,
            send_sem=send,
            recv_sem=recv,
            device_id={"fs": fs, "tp": tp},
            device_id_type=pl.DeviceIdType.MESH,
        )

    def arrived(dst, send, recv):
        remote(dst, dst, send, recv, pair, t).wait_recv()

    def sent(src, send, recv):
        remote(src, src, send, recv, pair, t).wait_send()

    def tok_copy(src, sem, to):
        return remote(tk.at[src], tk.at[src], sem, r_tok.at[src], f, to)

    loads = [
        pltpu.make_async_copy(src, dst, s_load.at[i])
        for i, (src, dst) in enumerate(
            (
                (tok_in, tok),
                (routes_in, routes),
                (weight_in, weight),
                (gain_in, gain),
                (eg_in, eg),
                (eu_in, eu),
                (ed_in, ed),
                (sg_in, sg),
                (su_in, su),
                (sd_in, sd),
            )
        )
    ]
    for load in loads:
        load.start()

    barrier = pltpu.get_barrier_semaphore()

    def greet(fs, tp):
        pl.semaphore_signal(
            barrier,
            inc=1,
            device_id={"fs": fs, "tp": tp},
            device_id_type=pl.DeviceIdType.MESH,
        )

    loop(1, F, lambda d: greet((f + d) % F, t))
    loop(1, T, lambda d: greet(f, (t + d) % T))

    def greet_rows(k):
        row = t * K + k

        @pl.when(row != f)
        def _():
            loop(1, T, lambda d: greet(row, (t + d) % T))

    loop(0, K, greet_rows)
    loads[0].wait()
    pl.semaphore_wait(barrier, F + T - 2 + (F - 1) * jnp.where(f // K == t, 0, 1))

    for o in range(1, T // 2):
        remote(tok, tk.at[t], s_tok.at[o], r_tok.at[t], f, (t + 2 * o) % T).start()
    remote(tok, tk.at[t], s_tok.at[T // 2], r_tok.at[t], f, t_pair).start()
    tk[t] = tok[...]

    for load in loads[1:3]:
        load.wait()
    experts = lax.broadcasted_iota(jnp.int32, (tok_count, E), 1)
    line = lax.broadcasted_iota(jnp.int32, (8, tok_count), 0)
    named_by = routes[...].astype(F32)
    turned = jnp.where(line == 0, named_by[0:1], named_by[1:2])
    turned = jnp.where(line == 2, weight[0:1, :], turned)
    turned = jnp.where(line == 3, weight[1:2, :], turned).T
    first, second = turned[:, 0:1].astype(jnp.int32), turned[:, 1:2].astype(jnp.int32)
    named = ((experts == first) | (experts == second)).astype(F32)
    rows = lax.broadcasted_iota(jnp.int32, (tok_count, tok_count), 0)
    cols = lax.broadcasted_iota(jnp.int32, (tok_count, tok_count), 1)
    before = (cols < rows).astype(F32).astype(BF)
    place = dot(before, named.astype(BF))
    slot_ids = lax.broadcasted_iota(jnp.int32, (tok_count, E * slots), 1)

    def pick_of(chosen):
        spot = jnp.sum(jnp.where(experts == chosen, place, 0.0), axis=1, keepdims=True)
        return slot_ids == chosen * slots + spot.astype(jnp.int32)

    pick0, pick1 = pick_of(first), pick_of(second)
    both = jnp.where(pick0 | pick1, 1.0, 0.0).astype(BF)

    packed = lax.dot_general(
        both, tok[...], (((0,), (0,)), ((), ())), preferred_element_type=F32
    ).astype(BF)
    disp[...] = packed.reshape(E, slots, quarter)
    port[t, f] = disp[g]

    def send_disp(d):
        e = (g + d) % G
        remote(
            disp.at[e], port.at[t, f], s_da.at[d], r_port.at[t, f], 2 * e + p, t
        ).start()

    loop(1, G, send_disp)

    def shared_copy(block, sems, to):
        return remote(sh.at[block], sh.at[block], sems, r_sh.at[block], to, t)

    def share_left(block):
        @pl.when(g > 0)
        def _():
            shared_copy(block, s_left.at[block // 2], f - 2).start()

    def share_right(block):
        @pl.when(g < G - 1)
        def _():
            shared_copy(block, s_right.at[block // 2], f + 2).start()

    def share_pair(block):
        shared_copy(block, s_shb.at[block // 2], pair).start()

    def relay(k):
        @pl.when(g - k >= 0)
        def _():
            block = f - 2 * k
            arrived(sh.at[block], s_right.at[0], r_sh.at[block])
            share_right(block)
            share_pair(block)

        @pl.when(g + k < G)
        def _():
            block = f + 2 * k
            arrived(sh.at[block], s_left.at[0], r_sh.at[block])
            share_left(block)
            share_pair(block)

    def pass_block(block):
        for d in range(1, T // 2):
            remote(
                port.at[t, block],
                port.at[t, block],
                s_out.at[d, block],
                r_port.at[t, block],
                f,
                (t + 2 * d) % T,
            ).start()
        remote(
            port.at[t, block],
            port.at[t, block],
            s_in.at[0, block],
            r_port.at[t, block],
            f,
            t_pair,
        ).start()

    def direct_block(d):
        block = ((g + G - d) % G) * 2 + p

        @pl.when(d > 0)
        def _():
            arrived(port.at[t, block], s_da.at[d], r_port.at[t, block])

        remote(
            port.at[t, block],
            port.at[t, block],
            s_db.at[d],
            r_port.at[t, block],
            pair,
            t,
        ).start()
        pass_block(block)

    def pair_block(d):
        block = ((g + G - d) % G) * 2 + 1 - p
        arrived(port.at[t, block], s_db.at[d], r_port.at[t, block])
        pass_block(block)

    def inner_block(d):
        for o in range(1, T // 2):
            src = (t + 2 * o) % T
            for q in (p, 1 - p):
                block = ((g + G - d) % G) * 2 + q
                arrived(port.at[src, block], s_out.at[o, block], r_port.at[src, block])
                remote(
                    port.at[src, block],
                    port.at[src, block],
                    s_in.at[o, block],
                    r_port.at[src, block],
                    f,
                    t_pair,
                ).start()

    loop(0, 1, direct_block)

    for load in loads[3:6]:
        load.wait()
    gains = jnp.broadcast_to(gain[...], (8, R)).T[:, 0:1]

    def fold(e):
        gate, up = eg[e] * gains, eu[e] * gains
        gu_send[2 * e] = left_halves(gate, up, half).astype(BF)
        gu_send[2 * e + 1] = right_halves(gate, up, half).astype(BF)

    loop(0, E, fold)
    gu[f] = gu_send[f]

    def send_gu(d):
        j = (f + d) % F
        remote(gu_send.at[j], gu.at[f], s_gu.at[d], r_gu.at[f], j, t).start()

    loop(1, F, send_gu)

    for load in loads[6:]:
        load.wait()

    def fold_down(e):
        top, low = ed[e, : R // 2], ed[e, R // 2 :]
        dn_send[2 * e] = left_halves(top, low, half).astype(BF)
        dn_send[2 * e + 1] = right_halves(top, low, half).astype(BF)

    loop(0, E, fold_down)
    sh[f, 0] = (sg[...] * gains).astype(BF)
    sh[f, 1] = (su[...] * gains).astype(BF)
    sh[f, 2] = sd[...].T.astype(BF)

    def down_copy(d):
        j = (f + d) % F
        return remote(
            dn_send.at[j], dn.at[f % K, t], s_dn.at[d], r_dn.at[f % K, t], j, f // K
        )

    mine = f // K == t

    @pl.when(mine)
    def _():
        dn[f % K, t] = dn_send[f]

    def send_down(d):
        @pl.when(jnp.logical_not((d == 0) & mine))
        def _():
            down_copy(d).start()

    loop(0, F, send_down)
    share_left(f)
    share_right(f)
    loop(1, G, direct_block)
    loop(0, G, pair_block)
    share_pair(f)
    loop(0, G, inner_block)

    for o in range(1, T // 2):
        src = (t + 2 * o) % T
        arrived(tk.at[src], s_tok.at[o], r_tok.at[src])
        tok_copy(src, s_tok.at[T // 2 + o], t_pair).start()

    def wait_gu(d):
        src = (f + d) % F
        arrived(gu.at[src], s_gu.at[d], r_gu.at[src])

    loop(1, F, wait_gu)

    def rows_of(q):
        return gu[q * K : (q + 1) * K].reshape(quarter, C)

    def hidden_of(block):
        total = jnp.zeros((slots, C), F32)
        squares = jnp.zeros((slots, 1), F32)
        for q in range(T):
            total = total + dot(port[q, block], rows_of(q))
            x = port[q, block].astype(F32)
            squares = squares + jnp.sum(x * x, axis=1, keepdims=True)
        total = total * lax.rsqrt(squares / width + EPS)
        return silu(total) * pltpu.roll(total, half, 1)

    def wait_inner(block):
        for o in range(T // 2):
            src = (t_pair + 2 * o) % T
            arrived(port.at[src, block], s_in.at[o, block], r_port.at[src, block])

    def expert_hidden(d):
        group = (g + G - d) % G
        wait_inner(2 * group)
        wait_inner(2 * group + 1)
        hid[t, group] = left_halves(
            hidden_of(2 * group), hidden_of(2 * group + 1), half
        ).astype(BF)
        for o in range(1, T):
            remote(
                hid.at[t, group],
                hid.at[t, group],
                s_hid.at[o, group],
                r_hid.at[t, group],
                f,
                (t + o) % T,
            ).start()

    loop(0, G, expert_hidden)

    loop(1, min(2, G), relay)

    def wait_down(k):
        for q in range(T):

            @pl.when(jnp.logical_not((t * K + k == f) & (t == q)))
            def _():
                arrived(dn.at[k, q], s_dn.at[0], r_dn.at[k, q])

    loop(0, K, wait_down)

    def place_down(k):
        for q in range(0, T, 2):
            a, b = dn[k, q].astype(F32), dn[k, q + 1].astype(F32)
            block = jnp.concatenate([left_halves(a, b, half), right_halves(a, b, half)], axis=0)
            dn_out[pl.ds(pl.multiple_of(k * R, R), R), q * half : (q + 2) * half] = block.astype(BF)

    loop(0, K, place_down)

    def near_copy(group):
        return remote(
            away.at[group], near.at[group], s_near.at[group], r_near.at[group], pair, t
        )

    def expert_out(d):
        group = (g + G - d) % G
        for o in range(1, T):
            src = (t + o) % T
            arrived(hid.at[src, group], s_hid.at[o, group], r_hid.at[src, group])
        out_a = jnp.zeros((slots, quarter), F32)
        out_b = jnp.zeros((slots, quarter), F32)
        for q in range(0, T, 2):
            a, b = hid[q, group].astype(F32), hid[q + 1, group].astype(F32)
            down = dn_out[:, q * half : (q + 2) * half]
            out_a = out_a + dot_nt(left_halves(a, b, half).astype(BF), down)
            out_b = out_b + dot_nt(right_halves(a, b, half).astype(BF), down)
        even, odd = out_a.astype(BF), out_b.astype(BF)
        keep[group] = jnp.where(p == 0, even, odd)
        away[group] = jnp.where(p == 0, odd, even)
        near_copy(group).start()

    loop(0, G, expert_out)
    loop(2, min(3, G), relay)

    def add_halves(d):
        group = (g + d) % G
        arrived(near.at[group], s_near.at[group], r_near.at[group])
        ret_send[group] = (keep[group].astype(F32) + near[group].astype(F32)).astype(BF)
        remote(
            ret_send.at[group], ret.at[g], s_ret.at[group], r_ret.at[g], 2 * group + p, t
        ).start()

    loop(1, G, add_halves)
    arrived(near.at[g], s_near.at[g], r_near.at[g])
    ret[g] = (keep[g].astype(F32) + near[g].astype(F32)).astype(BF)

    def wait_shared(d):
        block = ((g + G - d) % G) * 2 + 1 - p
        arrived(sh.at[block], s_shb.at[d], r_sh.at[block])

    loop(3, G, relay)
    loop(0, G, wait_shared)

    for o in range(T // 2):
        src = (t_pair + 2 * o) % T
        arrived(tk.at[src], s_tok.at[o], r_tok.at[src])
    squares = jnp.zeros((tok_count, 1), F32)
    for q in range(T):
        x = tk[q].astype(F32)
        squares = squares + jnp.sum(x * x, axis=1, keepdims=True)
    scale = lax.rsqrt(squares / width + EPS)
    for q in range(T):
        nm[q] = (tk[q].astype(F32) * scale).astype(BF)

    gate_sh = sh[:, 0].reshape(F * R, C)
    up_sh = sh[:, 1].reshape(F * R, C)
    down_sh = sh[:, 2].reshape(F * R, C)
    act = jnp.zeros((tok_count, C), F32)
    lin = jnp.zeros((tok_count, C), F32)
    for q in range(T):
        act = act + dot(nm[q], gate_sh[q * quarter : (q + 1) * quarter])
        lin = lin + dot(nm[q], up_sh[q * quarter : (q + 1) * quarter])
    hidden_sh = (silu(act) * lin).astype(BF)
    for q in range(T):
        part[q] = dot_nt(hidden_sh, down_sh[q * quarter : (q + 1) * quarter]).astype(BF)
    shr[t] = part[t]

    def send_part(d):
        q = (t + d) % T
        remote(part.at[q], shr.at[t], s_shr.at[d], r_shr.at[t], f, q).start()

    loop(1, T, send_part)

    for q in range(T):
        span = slice(q * quarter, (q + 1) * quarter)
        turned_gu = rows_of(q).astype(F32).T.astype(BF)
        gate_out[:, span] = turned_gu[:half]
        up_out[:, span] = turned_gu[half:]
        sd_out[:, span] = (
            sh[q * K : (q + 1) * K, 2].reshape(quarter, C).astype(F32).T.astype(BF)
        )
    sg_out[...] = sh[:, 0].reshape(F * R, C)
    su_out[...] = sh[:, 1].reshape(F * R, C)

    def wait_part(d):
        src = (t + d) % T
        arrived(shr.at[src], s_shr.at[d], r_shr.at[src])

    loop(1, T, wait_part)
    total = shr[0].astype(F32)
    for q in range(1, T):
        total = total + shr[q].astype(F32)

    def wait_ret(d):
        src = (g + d) % G
        arrived(ret.at[src], s_ret.at[src], r_ret.at[src])

    loop(1, G, wait_ret)
    outs = ret[...].reshape(E * slots, quarter)
    for k, pick in enumerate((pick0, pick1)):
        chosen = jnp.where(pick, 1.0, 0.0).astype(BF)
        total = total + turned[:, 2 + k : 3 + k] * dot(chosen, outs)
    mixed[...] = total.astype(BF)

    def done_tp(d):
        sent(tok, s_tok.at[d], r_tok.at[0])
        sent(part.at[0], s_shr.at[d], r_shr.at[0])

        def inner(group):
            sent(hid.at[t, group], s_hid.at[d, group], r_hid.at[0, 0])

        loop(0, G, inner)

    loop(1, T, done_tp)

    def done_fs(d):
        sent(gu_send.at[0], s_gu.at[d], r_gu.at[0])

    loop(1, F, done_fs)

    def done_down(d):
        @pl.when(jnp.logical_not((d == 0) & mine))
        def _():
            sent(dn_send.at[0], s_dn.at[d], r_dn.at[0, 0])

    loop(0, F, done_down)

    def done_groups(d):
        sent(sh.at[f], s_shb.at[d], r_sh.at[0])
        sent(disp.at[0], s_db.at[d], r_port.at[0, 0])
        sent(away.at[0], s_near.at[d], r_near.at[0])

        @pl.when(d > 0)
        def _():
            sent(disp.at[0], s_da.at[d], r_port.at[0, 0])
            sent(ret_send.at[0], s_ret.at[(g + d) % G], r_ret.at[0])

        @pl.when((d >= g) & (g > 0))
        def _():
            sent(sh.at[f], s_left.at[d], r_sh.at[0])

        @pl.when((d <= g) & (g < G - 1))
        def _():
            sent(sh.at[f], s_right.at[d], r_sh.at[0])

    loop(0, G, done_groups)

    def done_blocks(block):
        for o in range(T // 2):
            sent(disp.at[0], s_in.at[o, block], r_port.at[0, 0])
            if o > 0:
                sent(disp.at[0], s_out.at[o, block], r_port.at[0, 0])

    loop(0, F, done_blocks)


def hand_on(count, *refs):
    copies = [
        pltpu.make_async_copy(refs[i], refs[count + i], refs[-1].at[i])
        for i in range(count)
    ]
    for copy in copies:
        copy.start()
    for copy in copies:
        copy.wait()


def on_device(
    tokens,
    routes,
    route_weight,
    norm_gain,
    expert_gate,
    expert_up,
    expert_down,
    shared_gate,
    shared_up,
    shared_down,
):
    F = lax.axis_size("fs")
    T = lax.axis_size("tp")
    E, R, C = expert_gate.shape
    tok_count, quarter = tokens.shape
    pick_count = routes.shape[1]
    capacity = 2 * ((3 * tok_count * pick_count + 4 * E - 1) // (4 * E))
    slots = (capacity + 15) // 16 * 16
    G, K = F // 2, F // T
    vmem = pl.BlockSpec(memory_space=pltpu.VMEM)
    hbm = pl.BlockSpec(memory_space=pltpu.HBM)
    dma = pltpu.SemaphoreType.DMA
    shapes = [
        (tok_count, quarter),
        (C // 2, F * R),
        (C // 2, F * R),
        (K * R, T * C // 2),
        (F * R, C),
        (F * R, C),
        (C, F * R),
    ]
    scratch = [
        (T, tok_count, quarter),
        (T, tok_count, quarter),
        (F, R, C),
        (F, R, C),
        (F, R // 2, C),
        (K, T, R // 2, C),
        (F, 3, R, C),
        (E, slots, quarter),
        (T, F, slots, quarter),
        (T, G, slots, C),
        (G, slots, quarter),
        (G, slots, quarter),
        (G, slots, quarter),
        (G, slots, quarter),
        (E, slots, quarter),
        (T, tok_count, quarter),
        (T, tok_count, quarter),
    ]
    sems = [
        (T,), (T,), (F,), (F,), (F,), (K, T), (G,), (G,), (G,), (F,), (G,), (G,),
        (T // 2, F), (T // 2, F), (T, F), (T, G), (T, G), (G,), (G,), (G,), (E,), (T,), (T,),
    ]
    args = (
        tokens,
        routes.T,
        route_weight.T,
        norm_gain[None, :],
        expert_gate,
        expert_up,
        expert_down,
        shared_gate,
        shared_up,
        shared_down,
    )
    results = pl.pallas_call(
        functools.partial(kernel, F, T, slots),
        out_shape=[jax.ShapeDtypeStruct(s, BF) for s in shapes],
        in_specs=[hbm] * 10,
        out_specs=[vmem] * 7,
        scratch_shapes=[pltpu.VMEM(a.shape, a.dtype) for a in args]
        + [dma((len(args),))]
        + [pltpu.VMEM(s, BF) for s in scratch]
        + [dma(s) for s in sems],
        compiler_params=pltpu.CompilerParams(
            has_side_effects=True, collective_id=0, vmem_limit_bytes=24 * 1024 * 1024
        ),
    )(*[pltpu.with_memory_space_constraint(a, pltpu.HBM) for a in args])
    mixed, gate, up, down, sg, su, sd = pl.pallas_call(
        functools.partial(hand_on, 7),
        out_shape=[jax.ShapeDtypeStruct(s, BF) for s in shapes],
        in_specs=[vmem] * 7,
        out_specs=[hbm] * 7,
        scratch_shapes=[dma((7,))],
        compiler_params=pltpu.CompilerParams(vmem_limit_bytes=8 * 1024 * 1024),
    )(*results)
    return (mixed, gate.T[None], up.T[None], down[None], sg, su, sd)


def solution(mesh):
    in_specs = (
        P("fs", "tp"),
        P("fs", None),
        P("fs", None),
        P("fs"),
        P(None, "fs", "tp"),
        P(None, "fs", "tp"),
        P(None, "fs", "tp"),
        P("fs", "tp"),
        P("fs", "tp"),
        P("tp", "fs"),
    )
    out_specs = (
        P("fs", "tp"),
        P("fs", None, "tp"),
        P("fs", None, "tp"),
        P("fs", "tp", None),
        P(None, "tp"),
        P(None, "tp"),
        P("tp", None),
    )
    return jax.shard_map(
        on_device, mesh=mesh, in_specs=in_specs, out_specs=out_specs, check_vma=False
    )
```

```python
import functools

import jax
import jax.numpy as jnp
from jax import lax
from jax.experimental import pallas as pl
from jax.experimental.pallas import tpu as pltpu
from jax.sharding import PartitionSpec as P

EPS = 1e-06
BF = jnp.bfloat16
F32 = jnp.float32


def loop(low, high, body):
    def step(i, carry):
        body(i)
        return carry

    lax.fori_loop(low, high, step, 0)


def dot(a, b):
    return jnp.dot(a, b, preferred_element_type=F32)


def dot_nt(a, b):
    return lax.dot_general(a, b, (((1,), (1,)), ((), ())), preferred_element_type=F32)


def left_halves(a, b, half):
    lane = lax.broadcasted_iota(jnp.int32, a.shape, 1)
    return jnp.where(lane < half, a, pltpu.roll(b, half, 1))


def right_halves(a, b, half):
    lane = lax.broadcasted_iota(jnp.int32, a.shape, 1)
    return jnp.where(lane < half, pltpu.roll(a, half, 1), b)


def silu(v):
    return v / (1.0 + jnp.exp(-v))


def kernel(
    F,
    T,
    slots,
    tok_in,
    routes_in,
    weight_in,
    gain_in,
    eg_in,
    eu_in,
    ed_in,
    sg_in,
    su_in,
    sd_in,
    mixed,
    gate_out,
    up_out,
    dn_out,
    sg_out,
    su_out,
    sd_out,
    tok,
    routes,
    weight,
    gain,
    eg,
    eu,
    ed,
    sg,
    su,
    sd,
    s_load,
    tk,
    nm,
    gu_send,
    gu,
    dn_send,
    dn,
    sh,
    disp,
    port,
    hid,
    ret_send,
    ret,
    part,
    shr,
    s_tok,
    r_tok,
    s_gu,
    r_gu,
    f_gu,
    s_dn,
    r_dn,
    f_dn,
    s_left,
    s_right,
    s_shb,
    r_sh,
    s_da,
    p_out,
    p_in,
    r_port,
    s_out,
    s_in,
    r_hid,
    s_ret,
    r_ret,
    s_shr,
    r_shr,
):
    G = F // 2
    K = F // T
    H = T // 2
    E = eg.shape[0]
    R, C = eg.shape[1], eg.shape[2]
    half = C // 2
    tok_count = tok.shape[0]
    quarter = tok.shape[1]
    width = quarter * T
    f = lax.axis_index("fs")
    t = lax.axis_index("tp")
    g, p = f // 2, f % 2
    pair = g * 2 + (1 - p)
    y, c = t // 2, t % 2
    t_pair = y * 2 + (1 - c)
    home = f // K
    pieces = r_gu.shape[1]
    step = R // pieces
    mine = home == t

    def far_first(i):
        return jnp.where(2 * g < G, G - 1 - i, i)

    def near_first(i):
        return jnp.where(2 * g < G, i, G - 1 - i)

    def remote(src, dst, send, recv, fs, tp):
        return pltpu.make_async_remote_copy(
            src_ref=src,
            dst_ref=dst,
            send_sem=send,
            recv_sem=recv,
            device_id={"fs": fs, "tp": tp},
            device_id_type=pl.DeviceIdType.MESH,
        )

    def arrived(dst, send, recv):
        remote(dst, dst, send, recv, pair, t).wait_recv()

    def sent(src, send, recv):
        remote(src, src, send, recv, pair, t).wait_send()

    loads = [
        pltpu.make_async_copy(src, dst, s_load.at[i])
        for i, (src, dst) in enumerate(
            (
                (tok_in, tok),
                (routes_in, routes),
                (weight_in, weight),
                (gain_in, gain),
                (eg_in, eg),
                (eu_in, eu),
                (ed_in, ed),
                (sg_in, sg),
                (su_in, su),
                (sd_in, sd),
            )
        )
    ]
    for load in loads:
        load.start()

    barrier = pltpu.get_barrier_semaphore()

    def greet(fs, tp):
        pl.semaphore_signal(
            barrier,
            inc=1,
            device_id={"fs": fs, "tp": tp},
            device_id_type=pl.DeviceIdType.MESH,
        )

    loop(1, G, lambda d: greet(2 * ((g + d) % G) + p, t))
    greet(pair, t)
    loop(1, T, lambda d: greet(f, (t + d) % T))

    def greet_rows(i):
        row = t * K + 2 * i + p

        @pl.when(row != f)
        def _():
            loop(1, T, lambda d: greet(row, (t + d) % T))

    loop(0, K // 2, greet_rows)

    for load in loads[:3]:
        load.wait()
    experts = lax.broadcasted_iota(jnp.int32, (tok_count, E), 1)
    line = lax.broadcasted_iota(jnp.int32, (8, tok_count), 0)
    named_by = routes[...].astype(F32)
    turned = jnp.where(line == 0, named_by[0:1], named_by[1:2])
    turned = jnp.where(line == 2, weight[0:1, :], turned)
    turned = jnp.where(line == 3, weight[1:2, :], turned).T
    first, second = turned[:, 0:1].astype(jnp.int32), turned[:, 1:2].astype(jnp.int32)
    named = ((experts == first) | (experts == second)).astype(F32)
    rows = lax.broadcasted_iota(jnp.int32, (tok_count, tok_count), 0)
    cols = lax.broadcasted_iota(jnp.int32, (tok_count, tok_count), 1)
    before = (cols < rows).astype(F32).astype(BF)
    place = dot(before, named.astype(BF))
    slot_ids = lax.broadcasted_iota(jnp.int32, (tok_count, E * slots), 1)

    def spot_of(chosen):
        spot = jnp.sum(jnp.where(experts == chosen, place, 0.0), axis=1, keepdims=True)
        return spot.astype(jnp.int32)

    spot0, spot1 = spot_of(first), spot_of(second)
    pick0 = slot_ids == first * slots + spot0
    pick1 = slot_ids == second * slots + spot1
    both = jnp.where(pick0 | pick1, 1.0, 0.0).astype(BF)

    packed = lax.dot_general(
        both, tok[...], (((0,), (0,)), ((), ())), preferred_element_type=F32
    ).astype(BF)
    disp[...] = packed.reshape(E, slots, quarter)
    pl.semaphore_wait(barrier, G + T - 1 + (G - 1) * jnp.where(mine, 0, 1))

    def send_disp(i):
        e = far_first(i)

        @pl.when(e != g)
        def _():
            remote(
                disp.at[e], port.at[t, g], s_da.at[e], r_port.at[t, g], 2 * e + p, t
            ).start()

    loop(0, G, send_disp)
    port[t, g] = disp[g]

    def port_copy(src, group, sem, to):
        return remote(
            port.at[src, group], port.at[src, group], sem, r_port.at[src, group], f, to
        )

    def pass_block(group):
        for o in range(1, H):
            port_copy(t, group, p_out.at[o, group], (t + 2 * o) % T).start()
        port_copy(t, group, p_in.at[0, group], t_pair).start()

    pass_block(g)

    def tok_copy(src, sem, to):
        return remote(tk.at[src], tk.at[src], sem, r_tok.at[src], f, to)

    for o in range(1, H):
        remote(tok, tk.at[t], s_tok.at[o], r_tok.at[t], f, (t + 2 * o) % T).start()
    remote(tok, tk.at[t], s_tok.at[H], r_tok.at[t], f, t_pair).start()
    tk[t] = tok[...]

    def shared_copy(block, sems, to):
        return remote(sh.at[block], sh.at[block], sems, r_sh.at[block], to, t)

    def share_left(block):
        @pl.when(g > 0)
        def _():
            shared_copy(block, s_left.at[block // 2], f - 2).start()

    def share_right(block):
        @pl.when(g < G - 1)
        def _():
            shared_copy(block, s_right.at[block // 2], f + 2).start()

    def share_pair(block):
        shared_copy(block, s_shb.at[block // 2], pair).start()

    def relay_right(k):
        @pl.when(g - k >= 0)
        def _():
            block = f - 2 * k
            arrived(sh.at[block], s_right.at[0], r_sh.at[block])
            share_right(block)
            share_pair(block)

    def relay_left(k):
        @pl.when(g + k < G)
        def _():
            block = f + 2 * k
            arrived(sh.at[block], s_left.at[0], r_sh.at[block])
            share_left(block)
            share_pair(block)

    def relay_in(k):
        @pl.when(2 * g < G)
        def _():
            relay_right(k)

        @pl.when(2 * g >= G)
        def _():
            relay_left(k)

    def relay_out(k):
        @pl.when(2 * g < G)
        def _():
            relay_left(k)

        @pl.when(2 * g >= G)
        def _():
            relay_right(k)

    for load in loads[3:6]:
        load.wait()
    gains = jnp.broadcast_to(gain[...], (8, R)).T[:, 0:1]

    def rows_of(n):
        return pl.ds(pl.multiple_of(n * step, step), step)

    def send_gu(i):
        e = far_first(i)
        gu_send[e, :, :C] = (eg[e] * gains).astype(BF)
        gu_send[e, :, C:] = (eu[e] * gains).astype(BF)

        @pl.when(e != g)
        def _():
            def piece(n):
                remote(
                    gu_send.at[e, rows_of(n)],
                    gu.at[f, rows_of(n)],
                    s_gu.at[e, n],
                    r_gu.at[f, n],
                    2 * e + p,
                    t,
                ).start()

            loop(0, pieces, piece)

    loop(0, E, send_gu)
    gu[f] = gu_send[g]

    def cross(src, n):
        remote(
            gu.at[src, rows_of(n)],
            gu.at[src, rows_of(n)],
            f_gu.at[src // 2, n],
            r_gu.at[src, n],
            pair,
            t,
        ).start()

    loop(0, pieces, lambda n: cross(f, n))

    for load in loads[6:]:
        load.wait()
    sh[f, 0] = (sg[...] * gains).astype(BF)
    sh[f, 1] = (su[...] * gains).astype(BF)
    sh[f, 2] = sd[...].T.astype(BF)
    share_pair(f)

    def send_dn(i):
        e = far_first(i)
        dn_send[e] = ed[e].astype(BF)

        @pl.when(jnp.logical_not((e == g) & mine))
        def _():
            remote(
                dn_send.at[e], dn.at[f % K, t], s_dn.at[e], r_dn.at[f % K, t, 0], 2 * e + p, home
            ).start()

    loop(0, E, send_dn)

    @pl.when(mine)
    def _():
        dn[f % K, t] = dn_send[g]

    share_left(f)
    share_right(f)


    def take_block(i):
        group = near_first(i)

        @pl.when(group != g)
        def _():
            arrived(port.at[t, group], s_da.at[group], r_port.at[t, group])
            pass_block(group)

    loop(0, G, take_block)

    def inner_block(i):
        group = near_first(i)
        for o in range(1, H):
            src = (t + 2 * o) % T
            arrived(port.at[src, group], p_out.at[o, group], r_port.at[src, group])
            port_copy(src, group, p_in.at[o, group], t_pair).start()


    def take_near(i):
        src = 2 * jnp.where(2 * g < G, i, G - 1 - i) + p

        @pl.when(src != f)
        def _():
            def piece(n):
                arrived(gu.at[src, rows_of(n)], s_load.at[0], r_gu.at[src, n])
                cross(src, n)

            loop(0, pieces, piece)

    loop(0, G // 2, take_near)
    loop(0, G // 2, inner_block)

    def take_far(n):
        def block(i):
            src = 2 * jnp.where(2 * g < G, G // 2 + i, G // 2 - 1 - i) + p
            arrived(gu.at[src, rows_of(n)], s_load.at[0], r_gu.at[src, n])
            cross(src, n)

        loop(0, G // 2, block)

    loop(0, pieces // 2, take_far)
    loop(G // 2, G, inner_block)
    loop(pieces // 2, pieces, take_far)

    loop(1, G // 2, relay_in)

    for o in range(1, H):
        src = (t + 2 * o) % T
        arrived(tk.at[src], s_tok.at[o], r_tok.at[src])
        tok_copy(src, s_tok.at[H + o], t_pair).start()
    for o in range(H):
        src = (t_pair + 2 * o) % T
        arrived(tk.at[src], s_tok.at[o], r_tok.at[src])
    squares = jnp.zeros((tok_count, 1), F32)
    for q in range(T):
        x = tk[q].astype(F32)
        squares = squares + jnp.sum(x * x, axis=1, keepdims=True)
    scale = lax.rsqrt(squares / width + EPS)
    for q in range(T):
        nm[q] = (tk[q].astype(F32) * scale).astype(BF)
    def wait_inner(group):
        for o in range(H):
            src = (t_pair + 2 * o) % T
            arrived(port.at[src, group], p_in.at[o, group], r_port.at[src, group])

    loop(0, G, wait_inner)

    def crossed(i):
        src = 2 * near_first(i) + 1 - p
        loop(0, pieces, lambda n: arrived(gu.at[src, rows_of(n)], s_load.at[0], r_gu.at[src, n]))

    loop(0, G, crossed)

    def expert_hidden(i):
        group = far_first(i)
        total = jnp.zeros((slots, 2 * C), F32)
        squares = jnp.zeros((slots, 1), F32)
        for q in range(T):
            total = total + dot(
                port[q, group], gu[q * K : (q + 1) * K].reshape(quarter, 2 * C)
            )
            x = port[q, group].astype(F32)
            squares = squares + jnp.sum(x * x, axis=1, keepdims=True)
        total = total * lax.rsqrt(squares / width + EPS)
        hid[t, group] = (silu(total[:, :C]) * total[:, C:]).astype(BF)
        for o in range(1, H):
            remote(
                hid.at[t, group],
                hid.at[t, group],
                s_out.at[o, group],
                r_hid.at[t, group],
                f,
                (t + 2 * o) % T,
            ).start()
        remote(
            hid.at[t, group],
            hid.at[t, group],
            s_in.at[0, group],
            r_hid.at[t, group],
            f,
            t_pair,
        ).start()

    loop(0, G, expert_hidden)

    def hand_across(i, ref, recv, hand):
        k = 2 * i + p
        count = recv.shape[2]
        rows = R // count

        def piece(n):
            span = pl.ds(pl.multiple_of(n * rows, rows), rows)

            def chunk(q):
                part_of = ref.at[k, q, span]

                @pl.when(jnp.logical_not((t * K + k == f) & (q == t)))
                def _():
                    arrived(part_of, s_load.at[0], recv.at[k, q, n])

                remote(
                    part_of, part_of, hand.at[i, q, n], recv.at[k, q, n], pair, t
                ).start()

            loop(0, T, chunk)

        loop(0, count, piece)

    def handed(i, ref, recv):
        k = 2 * i + 1 - p
        count = recv.shape[2]
        rows = R // count

        def piece(n):
            span = pl.ds(pl.multiple_of(n * rows, rows), rows)
            loop(0, T, lambda q: arrived(ref.at[k, q, span], s_load.at[0], recv.at[k, q, n]))

        loop(0, count, piece)

    loop(0, K // 2, lambda i: hand_across(i, dn, r_dn, f_dn))
    loop(1, G // 2 + 1, relay_out)

    def pass_hidden(i):
        group = far_first(i)
        for o in range(1, H):
            src = (t + 2 * o) % T
            arrived(hid.at[src, group], s_out.at[o, group], r_hid.at[src, group])
            remote(
                hid.at[src, group],
                hid.at[src, group],
                s_in.at[o, group],
                r_hid.at[src, group],
                f,
                t_pair,
            ).start()

    loop(0, G, pass_hidden)
    loop(0, K // 2, lambda i: handed(i, dn, r_dn))

    def expert_out(i):
        group = far_first(i)
        for o in range(H):
            src = (t_pair + 2 * o) % T
            arrived(hid.at[src, group], s_in.at[o, group], r_hid.at[src, group])
        total = jnp.zeros((slots, quarter), F32)
        for q in range(T):
            total = total + dot_nt(hid[q, group], dn[:, q].reshape(K * R, C))
        ret_send[group] = total.astype(BF)

        @pl.when(group != g)
        def _():
            remote(
                ret_send.at[group], ret.at[g], s_ret.at[group], r_ret.at[g], 2 * group + p, t
            ).start()

    loop(0, G, expert_out)
    ret[g] = ret_send[g]

    loop(G // 2 + 1, G, relay_out)
    loop(G // 2, G, relay_in)

    def place_down(k):
        for q in range(0, T, 2):
            a, b = dn[k, q].astype(F32), dn[k, q + 1].astype(F32)
            block = jnp.where(
                p == 0, left_halves(a, b, half), right_halves(a, b, half)
            )
            dn_out[pl.ds(pl.multiple_of(k * R, R), R), q * half : (q + 2) * half] = block.astype(BF)

    loop(0, K, place_down)

    def wait_shared(d):
        block = ((g + G - d) % G) * 2 + 1 - p
        arrived(sh.at[block], s_shb.at[d], r_sh.at[block])

    loop(0, G, wait_shared)

    gate_sh = sh[:, 0].reshape(F * R, C)
    up_sh = sh[:, 1].reshape(F * R, C)
    down_sh = sh[:, 2].reshape(F * R, C)
    act = jnp.zeros((tok_count, C), F32)
    lin = jnp.zeros((tok_count, C), F32)
    for q in range(T):
        act = act + dot(nm[q], gate_sh[q * quarter : (q + 1) * quarter])
        lin = lin + dot(nm[q], up_sh[q * quarter : (q + 1) * quarter])
    hidden_sh = (silu(act) * lin).astype(BF)
    for q in range(T):
        part[q] = dot_nt(hidden_sh, down_sh[q * quarter : (q + 1) * quarter]).astype(BF)
    shr[t] = part[t]

    def send_part(d):
        q = (t + d) % T
        remote(part.at[q], shr.at[t], s_shr.at[d], r_shr.at[t], f, q).start()

    loop(1, T, send_part)

    for q in range(T):
        span = slice(q * quarter, (q + 1) * quarter)
        sd_out[:, span] = (
            sh[q * K : (q + 1) * K, 2].reshape(quarter, C).astype(F32).T.astype(BF)
        )
    sg_out[...] = sh[:, 0].reshape(F * R, C)
    su_out[...] = sh[:, 1].reshape(F * R, C)

    for q in range(T):
        span = slice(q * quarter, (q + 1) * quarter)
        whole = gu[q * K : (q + 1) * K].reshape(quarter, 2 * C).astype(F32)
        gate, up = whole[:, :C].T, whole[:, C:].T
        gate_out[:, span] = jnp.where(p == 0, gate[:half], gate[half:]).astype(BF)
        up_out[:, span] = jnp.where(p == 0, up[:half], up[half:]).astype(BF)

    def wait_ret(d):
        src = (g + d) % G
        arrived(ret.at[src], s_ret.at[src], r_ret.at[src])

    loop(1, G, wait_ret)
    outs = ret[...].reshape(E * slots, quarter)
    routed = jnp.zeros((tok_count, quarter), F32)
    for k, pick in enumerate((pick0, pick1)):
        chosen = jnp.where(pick, 1.0, 0.0).astype(BF)
        routed = routed + turned[:, 2 + k : 3 + k] * dot(chosen, outs)

    def wait_part(d):
        src = (t + d) % T
        arrived(shr.at[src], s_shr.at[d], r_shr.at[src])

    loop(1, T, wait_part)
    total = shr[0].astype(F32)
    for q in range(1, T):
        total = total + shr[q].astype(F32)
    mixed[...] = (total + routed).astype(BF)

    def done_tp(d):
        sent(tok, s_tok.at[d], r_tok.at[0])
        sent(part.at[0], s_shr.at[d], r_shr.at[0])

    loop(1, T, done_tp)

    def done_experts(e):
        @pl.when(jnp.logical_not((e == g) & mine))
        def _():
            sent(dn_send.at[0], s_dn.at[e], r_dn.at[0, 0, 0])

        @pl.when(e != g)
        def _():
            loop(0, pieces, lambda n: sent(gu_send.at[0, :step], s_gu.at[e, n], r_gu.at[0, 0]))
            sent(disp.at[0], s_da.at[e], r_port.at[0, 0])
            sent(ret_send.at[0], s_ret.at[e], r_ret.at[0])

        loop(0, pieces, lambda n: sent(gu.at[0, :step], f_gu.at[e, n], r_gu.at[0, 0]))
        for o in range(1, H):
            sent(disp.at[0], p_out.at[o, e], r_port.at[0, 0])
            sent(hid.at[0, 0], s_out.at[o, e], r_hid.at[0, 0])
        for o in range(H):
            sent(disp.at[0], p_in.at[o, e], r_port.at[0, 0])
            sent(hid.at[0, 0], s_in.at[o, e], r_hid.at[0, 0])

    loop(0, G, done_experts)

    def done_hands(i):
        def chunk(q):
            sent(dn.at[0, 0], f_dn.at[i, q, 0], r_dn.at[0, 0, 0])

        loop(0, T, chunk)

    loop(0, K // 2, done_hands)

    def done_groups(d):
        sent(sh.at[f], s_shb.at[d], r_sh.at[0])

        @pl.when((d >= g) & (g > 0))
        def _():
            sent(sh.at[f], s_left.at[d], r_sh.at[0])

        @pl.when((d <= g) & (g < G - 1))
        def _():
            sent(sh.at[f], s_right.at[d], r_sh.at[0])

    loop(0, G, done_groups)


def hand_on(count, *refs):
    copies = [
        pltpu.make_async_copy(refs[i], refs[count + i], refs[-1].at[i])
        for i in range(count)
    ]
    for copy in copies:
        copy.start()
    for copy in copies:
        copy.wait()


def on_device(
    tokens,
    routes,
    route_weight,
    norm_gain,
    expert_gate,
    expert_up,
    expert_down,
    shared_gate,
    shared_up,
    shared_down,
):
    F = lax.axis_size("fs")
    T = lax.axis_size("tp")
    E, R, C = expert_gate.shape
    tok_count, quarter = tokens.shape
    pick_count = routes.shape[1]
    capacity = 2 * ((3 * tok_count * pick_count + 4 * E - 1) // (4 * E))
    slots = (capacity + 15) // 16 * 16
    G, K = F // 2, F // T
    vmem = pl.BlockSpec(memory_space=pltpu.VMEM)
    hbm = pl.BlockSpec(memory_space=pltpu.HBM)
    dma = pltpu.SemaphoreType.DMA
    shapes = [
        (tok_count, quarter),
        (C // 2, F * R),
        (C // 2, F * R),
        (K * R, T * C // 2),
        (F * R, C),
        (F * R, C),
        (C, F * R),
    ]
    H, N = T // 2, max(R // 64, 1)
    scratch = [
        (T, tok_count, quarter),
        (T, tok_count, quarter),
        (E, R, 2 * C),
        (F, R, 2 * C),
        (E, R, C),
        (K, T, R, C),
        (F, 3, R, C),
        (E, slots, quarter),
        (T, G, slots, quarter),
        (T, G, slots, C),
        (G, slots, quarter),
        (G, slots, quarter),
        (T, tok_count, quarter),
        (T, tok_count, quarter),
    ]
    sems = [
        (T,), (T,), (E, N), (F, N), (G, N), (E,), (K, T, 1), (K // 2, T, 1),
        (G,), (G,), (G,), (F,), (E,), (H, G), (H, G), (T, G),
        (H, G), (H, G), (T, G), (G,), (G,), (T,), (T,),
    ]
    args = (
        tokens,
        routes.T,
        route_weight.T,
        norm_gain[None, :],
        expert_gate,
        expert_up,
        expert_down,
        shared_gate,
        shared_up,
        shared_down,
    )
    results = pl.pallas_call(
        functools.partial(kernel, F, T, slots),
        out_shape=[jax.ShapeDtypeStruct(s, BF) for s in shapes],
        in_specs=[hbm] * 10,
        out_specs=[vmem] * 7,
        scratch_shapes=[pltpu.VMEM(a.shape, a.dtype) for a in args]
        + [dma((len(args),))]
        + [pltpu.VMEM(s, BF) for s in scratch]
        + [dma(s) for s in sems],
        compiler_params=pltpu.CompilerParams(
            has_side_effects=True, collective_id=0, vmem_limit_bytes=32 * 1024 * 1024
        ),
    )(*[pltpu.with_memory_space_constraint(a, pltpu.HBM) for a in args])
    mixed, gate, up, down, sg, su, sd = pl.pallas_call(
        functools.partial(hand_on, 7),
        out_shape=[jax.ShapeDtypeStruct(s, BF) for s in shapes],
        in_specs=[vmem] * 7,
        out_specs=[hbm] * 7,
        scratch_shapes=[dma((7,))],
        compiler_params=pltpu.CompilerParams(vmem_limit_bytes=8 * 1024 * 1024),
    )(*results)
    return (mixed, gate.T[None], up.T[None], down[None], sg, su, sd)


def solution(mesh):
    in_specs = (
        P("fs", "tp"),
        P("fs", None),
        P("fs", None),
        P("fs"),
        P(None, "fs", "tp"),
        P(None, "fs", "tp"),
        P(None, "fs", "tp"),
        P("fs", "tp"),
        P("fs", "tp"),
        P("tp", "fs"),
    )
    out_specs = (
        P("fs", "tp"),
        P("fs", None, "tp"),
        P("fs", None, "tp"),
        P("fs", "tp", None),
        P(None, "tp"),
        P(None, "tp"),
        P("tp", None),
    )
    return jax.shard_map(
        on_device, mesh=mesh, in_specs=in_specs, out_specs=out_specs, check_vma=False
    )
```

```python
import functools

import jax
import jax.numpy as jnp
from jax import lax
from jax.experimental import pallas as pl
from jax.experimental.pallas import tpu as pltpu
from jax.sharding import PartitionSpec as P

EPS = 1e-06
BF = jnp.bfloat16
F32 = jnp.float32


def loop(low, high, body):
    def step(i, carry):
        body(i)
        return carry

    lax.fori_loop(low, high, step, 0)


def dot(a, b):
    return jnp.dot(a, b, preferred_element_type=F32)


def dot_nt(a, b):
    return lax.dot_general(a, b, (((1,), (1,)), ((), ())), preferred_element_type=F32)


def left_halves(a, b, half):
    lane = lax.broadcasted_iota(jnp.int32, a.shape, 1)
    return jnp.where(lane < half, a, pltpu.roll(b, half, 1))


def right_halves(a, b, half):
    lane = lax.broadcasted_iota(jnp.int32, a.shape, 1)
    return jnp.where(lane < half, pltpu.roll(a, half, 1), b)


def silu(v):
    return v / (1.0 + jnp.exp(-v))


def kernel(
    F,
    T,
    slots,
    tok_in,
    routes_in,
    weight_in,
    gain_in,
    eg_in,
    eu_in,
    ed_in,
    sg_in,
    su_in,
    sd_in,
    mixed,
    gate_out,
    up_out,
    dn_out,
    sg_out,
    su_out,
    sd_out,
    tok,
    routes,
    weight,
    gain,
    eg,
    eu,
    ed,
    sg,
    su,
    sd,
    s_load,
    tk,
    nm,
    gu_send,
    gu,
    dn_send,
    dn,
    sh,
    disp,
    port,
    hid,
    ret_send,
    ret,
    hsh,
    sdx,
    raw,
    gw_send,
    meta_send,
    meta,
    s_tok,
    r_tok,
    s_gu,
    r_gu,
    x_gu,
    f_gu,
    s_dn,
    r_dn,
    x_dn,
    f_dn,
    s_left,
    s_right,
    s_shb,
    r_sh,
    r_shp,
    s_da,
    p_out,
    p_in,
    r_port,
    x_port,
    s_raw,
    r_raw,
    s_meta,
    r_meta,
    s_gw,
    s_out,
    s_in,
    r_hid,
    s_ret,
    r_ret,
    s_hsh,
    r_hsh,
    s_sdx,
    r_sdx,
):
    G = F // 2
    K = F // T
    H = T // 2
    E = eg.shape[0]
    R, C = eg.shape[1], eg.shape[2]
    half = C // 2
    tok_count = tok.shape[0]
    quarter = tok.shape[1]
    width = quarter * T
    f = lax.axis_index("fs")
    t = lax.axis_index("tp")
    g, p = f // 2, f % 2
    pair = g * 2 + (1 - p)
    y, c = t // 2, t % 2
    t_pair = y * 2 + (1 - c)
    home = f // K
    pieces = r_gu.shape[1]
    D = G // 2
    step = R // pieces
    mine = home == t

    def far_first(i):
        return jnp.where(2 * g < G, G - 1 - i, i)

    def near_first(i):
        return jnp.where(2 * g < G, i, G - 1 - i)

    def send_order(i):
        return jnp.where(i < G // 2, near_first(i), far_first(i - G // 2))

    left = 2 * g < G
    depth = jnp.where(left, g, G - 1 - g)
    gateway = jnp.where(left, D, D - 1)

    def remote(src, dst, send, recv, fs, tp):
        return pltpu.make_async_remote_copy(
            src_ref=src,
            dst_ref=dst,
            send_sem=send,
            recv_sem=recv,
            device_id={"fs": fs, "tp": tp},
            device_id_type=pl.DeviceIdType.MESH,
        )

    def arrived(dst, send, recv):
        remote(dst, dst, send, recv, pair, t).wait_recv()

    def sent(src, send, recv):
        remote(src, src, send, recv, pair, t).wait_send()

    loads = [
        pltpu.make_async_copy(src, dst, s_load.at[i])
        for i, (src, dst) in enumerate(
            (
                (tok_in, tok),
                (routes_in, routes),
                (weight_in, weight),
                (gain_in, gain),
                (eg_in, eg),
                (eu_in, eu),
                (ed_in, ed),
                (sg_in, sg),
                (su_in, su),
                (sd_in, sd),
            )
        )
    ]
    for load in loads:
        load.start()

    barrier = pltpu.get_barrier_semaphore()

    def greet(fs, tp):
        pl.semaphore_signal(
            barrier,
            inc=1,
            device_id={"fs": fs, "tp": tp},
            device_id_type=pl.DeviceIdType.MESH,
        )

    loop(1, G, lambda d: greet(2 * ((g + d) % G) + p, t))
    greet(pair, t)
    loop(1, T, lambda d: greet(f, (t + d) % T))

    def greet_rows(i):
        row = t * K + 2 * i + p

        @pl.when(row != f)
        def _():
            loop(1, T, lambda d: greet(row, (t + d) % T))

    loop(0, K // 2, greet_rows)

    for load in loads[:2]:
        load.wait()
    named_by = routes[...].astype(F32)
    line = lax.broadcasted_iota(jnp.int32, (8, tok_count), 0)
    meta_send[...] = jnp.where(line == 0, named_by[0:1], named_by[1:2])
    rows = lax.broadcasted_iota(jnp.int32, (tok_count, tok_count), 0)
    cols = lax.broadcasted_iota(jnp.int32, (tok_count, tok_count), 1)
    after = (rows < cols).astype(F32).astype(BF)
    slot_rows = lax.broadcasted_iota(jnp.int32, (slots, tok_count), 0)

    def pack(e, names, block):
        chosen = e.astype(F32)
        held = ((names[0:1] == chosen) | (names[1:2] == chosen)).astype(F32)
        spots = dot(jnp.broadcast_to(held, (16, tok_count)).astype(BF), after)
        here = (slot_rows == spots[0:1].astype(jnp.int32)) & (held > 0.5)
        return dot(here.astype(F32).astype(BF), block).astype(BF)

    def at_depth(i):
        return jnp.where(left, i, G - 1 - i)

    for i in range(D):
        disp[i] = pack(at_depth(i), meta_send[...], tok[...])
    pl.semaphore_wait(barrier, G + T - 1 + (G - 1) * jnp.where(mine, 0, 1))
    remote(tok, raw.at[depth], s_raw.at[0], r_raw.at[depth], 2 * gateway + p, t).start()
    remote(
        meta_send, meta.at[depth], s_meta.at[0], r_meta.at[depth], 2 * gateway + p, t
    ).start()

    def send_disp(i):
        @pl.when(i != depth)
        def _():
            remote(
                disp.at[i],
                port.at[t, g],
                s_da.at[0],
                r_port.at[0, g],
                2 * at_depth(i) + p,
                t,
            ).start()

    loop(0, D, send_disp)
    port[t, g] = disp[depth]

    def port_copy(src, group, sem, recv, to):
        return remote(port.at[src, group], port.at[src, group], sem, recv, f, to)

    def pass_block(group):
        for o in range(1, H):
            port_copy(
                t, group, p_out.at[0], r_port.at[H - o, group], (t + 2 * o) % T
            ).start()
        port_copy(t, group, p_in.at[0], x_port.at[0], t_pair).start()

    pass_block(g)

    def tok_copy(src, sem, to):
        return remote(tk.at[src], tk.at[src], sem, r_tok.at[src], f, to)

    for o in range(1, H):
        remote(tok, tk.at[t], s_tok.at[0], r_tok.at[t], f, (t + 2 * o) % T).start()
    remote(tok, tk.at[t], s_tok.at[0], r_tok.at[t], f, t_pair).start()
    tk[t] = tok[...]

    def shared_copy(block, i, sems, recv, to):
        return remote(sh.at[block, i], sh.at[block, i], sems, recv, to, t)

    def share_left(block, i):
        @pl.when(g > 0)
        def _():
            shared_copy(block, i, s_left.at[block // 2], r_sh.at[block // 2, i], f - 2).start()

    def share_right(block, i):
        @pl.when(g < G - 1)
        def _():
            shared_copy(block, i, s_right.at[block // 2], r_sh.at[block // 2, i], f + 2).start()

    def share_pair(block, i):
        shared_copy(block, i, s_shb.at[0], r_shp.at[block // 2, (i + 1) // 2], pair).start()

    def spread(block):
        @pl.when(block // K != t)
        def _():
            remote(
                sh.at[block, 0],
                sdx.at[t, block % K],
                s_sdx.at[0],
                r_sdx.at[0],
                f,
                block // K,
            ).start()

    def relay_right(k):
        @pl.when(g - k >= 0)
        def _():
            block = f - 2 * k

            def piece(i):
                arrived(sh.at[block, i], s_load.at[0], r_sh.at[block // 2, i])
                share_right(block, i)
                share_pair(block, i)

            loop(0, 3, piece)
            spread(block)

    def relay_left(k):
        @pl.when(g + k < G)
        def _():
            block = f + 2 * k

            def piece(i):
                arrived(sh.at[block, i], s_load.at[0], r_sh.at[block // 2, i])
                share_left(block, i)
                share_pair(block, i)

            loop(0, 3, piece)
            spread(block)

    def relay_in(k):
        @pl.when(2 * g < G)
        def _():
            relay_right(k)

        @pl.when(2 * g >= G)
        def _():
            relay_left(k)

    def relay_out(k):
        @pl.when(2 * g < G)
        def _():
            relay_left(k)

        @pl.when(2 * g >= G)
        def _():
            relay_right(k)

    for load in loads[2:6]:
        load.wait()
    gains = jnp.broadcast_to(gain[...], (8, R)).T[:, 0:1]

    def rows_of(n):
        return pl.ds(pl.multiple_of(n * step, step), step)

    def send_gu(i):
        e = send_order(i)
        gu_send[e, :, :C] = (eg[e] * gains).astype(BF)
        gu_send[e, :, C:] = (eu[e] * gains).astype(BF)

        @pl.when(e != g)
        def _():
            def piece(n):
                remote(
                    gu_send.at[e, rows_of(n)],
                    gu.at[f, rows_of(n)],
                    s_gu.at[0],
                    r_gu.at[g, n],
                    2 * e + p,
                    t,
                ).start()

            loop(0, pieces, piece)

    loop(0, E, send_gu)
    gu[f] = gu_send[g]

    def cross(src, n):
        remote(
            gu.at[src, rows_of(n)],
            gu.at[src, rows_of(n)],
            f_gu.at[0],
            x_gu.at[0],
            pair,
            t,
        ).start()

    loop(0, pieces, lambda n: cross(f, n))

    for load in loads[6:]:
        load.wait()
    sh[f, 0] = sd[...].T.astype(BF)
    sh[f, 1] = (sg[...] * gains).astype(BF)
    sh[f, 2] = (su[...] * gains).astype(BF)
    spread(f)
    loop(0, 3, lambda i: share_pair(f, i))

    def take_block(group):
        arrived(port.at[t, group], s_load.at[0], r_port.at[0, group])
        pass_block(group)

    def take_side(i):
        @pl.when(i != depth)
        def _():
            take_block(at_depth(i))

    def take_other(i):
        take_block(at_depth(G - 1 - i))

    def open_block(i):
        group = at_depth(G - 1 - i)
        arrived(raw.at[i], s_load.at[0], r_raw.at[i])
        arrived(meta.at[i], s_load.at[0], r_meta.at[i])
        for k in range(D - 1):
            gw_send[i, k] = pack(at_depth(k), meta[i], raw[i])
            remote(
                gw_send.at[i, k],
                port.at[t, group],
                s_gw.at[0],
                r_port.at[0, group],
                2 * at_depth(k) + p,
                t,
            ).start()
        port[t, group] = pack(g, meta[i], raw[i])
        pass_block(group)

    def inner_block(i):
        group = near_first(i)
        for o in range(1, H):
            src = (t + 2 * o) % T
            arrived(port.at[src, group], s_load.at[0], r_port.at[o, group])
            port_copy(src, group, p_in.at[0], x_port.at[0], t_pair).start()


    def take_near(i):
        src = 2 * jnp.where(2 * g < G, i, G - 1 - i) + p

        @pl.when(src != f)
        def _():
            def piece(n):
                arrived(gu.at[src, rows_of(n)], s_load.at[0], r_gu.at[src // 2, n])
                cross(src, n)

            loop(0, pieces, piece)


    def take_far(n):
        def block(i):
            src = 2 * jnp.where(2 * g < G, G // 2 + i, G // 2 - 1 - i) + p
            arrived(gu.at[src, rows_of(n)], s_load.at[0], r_gu.at[src // 2, n])
            cross(src, n)

        loop(0, G // 2, block)


    def expert_hidden(i):
        group = near_first(i)
        total = jnp.zeros((slots, 2 * C), F32)
        squares = jnp.zeros((slots, 1), F32)
        for q in range(T):
            total = total + dot(
                port[q, group], gu[q * K : (q + 1) * K].reshape(quarter, 2 * C)
            )
            x = port[q, group].astype(F32)
            squares = squares + jnp.sum(x * x, axis=1, keepdims=True)
        total = total * lax.rsqrt(squares / width + EPS)
        hid[t, group] = (silu(total[:, :C]) * total[:, C:]).astype(BF)
        for o in range(1, H):
            remote(
                hid.at[t, group],
                hid.at[t, group],
                s_out.at[0],
                r_hid.at[H - o, group],
                f,
                (t + 2 * o) % T,
            ).start()
        remote(
            hid.at[t, group],
            hid.at[t, group],
            s_in.at[0],
            r_hid.at[0, group],
            f,
            t_pair,
        ).start()


    def hand_across(i):
        k = 2 * i + p

        def chunk(q):
            @pl.when(jnp.logical_not((t * K + k == f) & (q == t)))
            def _():
                arrived(dn.at[k, q], s_load.at[0], r_dn.at[i, q])

            remote(dn.at[k, q], dn.at[k, q], f_dn.at[0], x_dn.at[0], pair, t).start()

        loop(0, T, chunk)

    def pass_hidden(i):
        group = near_first(i)
        for o in range(1, H):
            src = (t + 2 * o) % T
            arrived(hid.at[src, group], s_load.at[0], r_hid.at[o, group])
            remote(
                hid.at[src, group],
                hid.at[src, group],
                s_in.at[0],
                r_hid.at[0, group],
                f,
                t_pair,
            ).start()


    def expert_out(i):
        group = near_first(i)
        arrived(hid.at[:H, group], s_load.at[0], r_hid.at[0, group])
        total = jnp.zeros((slots, quarter), F32)
        for q in range(T):
            total = total + dot_nt(hid[q, group], dn[:, q].reshape(K * R, C))
        ret_send[group] = total.astype(BF)

        @pl.when(group != g)
        def _():
            remote(
                ret_send.at[group], ret.at[g], s_ret.at[0], r_ret.at[0], 2 * group + p, t
            ).start()


    at_gate = depth == D - 1

    @pl.when(at_gate)
    def _():
        loop(0, D, lambda i: open_block(D - 1 - i))

    loop(0, D, take_side)

    def send_dn(i):
        e = send_order(i)
        dn_send[e] = ed[e].astype(BF)

        @pl.when(jnp.logical_not((e == g) & mine))
        def _():
            remote(
                dn_send.at[e], dn.at[f % K, t], s_dn.at[0], r_dn.at[f % K // 2, t], 2 * e + p, home
            ).start()

    loop(0, E, send_dn)

    @pl.when(mine)
    def _():
        dn[f % K, t] = dn_send[g]

    loop(0, 3, lambda i: share_left(f, i))
    loop(0, 3, lambda i: share_right(f, i))


    loop(0, G // 2, take_near)

    @pl.when(jnp.logical_not(at_gate))
    def _():
        loop(0, D, lambda i: take_other(D - 1 - i))

    loop(0, pieces, take_far)
    loop(0, G, inner_block)
    loop(0, K // 2, hand_across)
    loop(1, G // 2, relay_in)

    for o in range(1, H):
        src = (t + 2 * o) % T
        arrived(tk.at[src], s_load.at[0], r_tok.at[src])
        tok_copy(src, s_tok.at[0], t_pair).start()
    for o in range(H):
        src = (t_pair + 2 * o) % T
        arrived(tk.at[src], s_load.at[0], r_tok.at[src])
    squares = jnp.zeros((tok_count, 1), F32)
    for q in range(T):
        x = tk[q].astype(F32)
        squares = squares + jnp.sum(x * x, axis=1, keepdims=True)
    scale = lax.rsqrt(squares / width + EPS)
    for q in range(T):
        nm[q] = (tk[q].astype(F32) * scale).astype(BF)
    arrived(port.at[:H], s_load.at[0], x_port.at[0])
    arrived(gu.at[:G], s_load.at[0], x_gu.at[0])
    loop(0, G, expert_hidden)
    loop(1, min(2, G), relay_out)
    loop(0, G, pass_hidden)
    at_end = (g == 0) | (g == G - 1)

    @pl.when(jnp.logical_not(at_end))
    def _():
        loop(2, G // 2 + 1, relay_out)

    arrived(dn.at[: K // 2], s_load.at[0], x_dn.at[0])
    loop(0, G, expert_out)
    ret[g] = ret_send[g]

    @pl.when(at_end)
    def _():
        loop(2, G // 2 + 1, relay_out)

    loop(G // 2 + 1, G, relay_out)
    loop(G // 2, G, relay_in)

    def place_down(k):
        for q in range(0, T, 2):
            a, b = dn[k, q].astype(F32), dn[k, q + 1].astype(F32)
            block = jnp.where(
                p == 0, left_halves(a, b, half), right_halves(a, b, half)
            )
            dn_out[pl.ds(pl.multiple_of(k * R, R), R), q * half : (q + 2) * half] = block.astype(BF)

    loop(0, K, place_down)

    def wait_down(i):
        block = near_first(i) * 2 + 1 - p
        arrived(sh.at[block, 0], s_load.at[0], r_shp.at[block // 2, 0])
        spread(block)
        arrived(sh.at[block, 1:3], s_load.at[0], r_shp.at[block // 2, 1])

    loop(0, G, wait_down)

    gate_sh = sh[:, 1].reshape(F * R, C)
    up_sh = sh[:, 2].reshape(F * R, C)
    act = jnp.zeros((tok_count, C), F32)
    lin = jnp.zeros((tok_count, C), F32)
    for q in range(T):
        act = act + dot(nm[q], gate_sh[q * quarter : (q + 1) * quarter])
        lin = lin + dot(nm[q], up_sh[q * quarter : (q + 1) * quarter])
    hsh[t] = (silu(act) * lin).astype(BF)

    def send_hsh(d):
        remote(
            hsh.at[t], hsh.at[t], s_hsh.at[0], r_hsh.at[0], f, (t + d) % T
        ).start()

    loop(1, T, send_hsh)

    def keep_down(k):
        sdx[t, k] = sh[t * K + k, 0]

    loop(0, K, keep_down)

    for q in range(T):
        span = slice(q * quarter, (q + 1) * quarter)
        sd_out[:, span] = (
            sh[q * K : (q + 1) * K, 0].reshape(quarter, C).astype(F32).T.astype(BF)
        )
    sg_out[...] = sh[:, 1].reshape(F * R, C)
    su_out[...] = sh[:, 2].reshape(F * R, C)

    for q in range(T):
        span = slice(q * quarter, (q + 1) * quarter)
        whole = gu[q * K : (q + 1) * K].reshape(quarter, 2 * C).astype(F32)
        gate, up = whole[:, :C].T, whole[:, C:].T
        gate_out[:, span] = jnp.where(p == 0, gate[:half], gate[half:]).astype(BF)
        up_out[:, span] = jnp.where(p == 0, up[:half], up[half:]).astype(BF)

    experts = lax.broadcasted_iota(jnp.int32, (tok_count, E), 1)
    turned = jnp.where(line == 2, weight[0:1, :], meta_send[...])
    turned = jnp.where(line == 3, weight[1:2, :], turned).T
    first, second = turned[:, 0:1].astype(jnp.int32), turned[:, 1:2].astype(jnp.int32)
    named = ((experts == first) | (experts == second)).astype(F32)
    before = (cols < rows).astype(F32).astype(BF)
    place = dot(before, named.astype(BF))
    slot_ids = lax.broadcasted_iota(jnp.int32, (tok_count, E * slots), 1)

    def pick_of(chosen):
        spot = jnp.sum(jnp.where(experts == chosen, place, 0.0), axis=1, keepdims=True)
        return slot_ids == chosen * slots + spot.astype(jnp.int32)

    pick0, pick1 = pick_of(first), pick_of(second)

    arrived(ret.at[: G - 1], s_load.at[0], r_ret.at[0])
    outs = ret[...].reshape(E * slots, quarter)
    routed = jnp.zeros((tok_count, quarter), F32)
    for k, pick in enumerate((pick0, pick1)):
        chosen = jnp.where(pick, 1.0, 0.0).astype(BF)
        routed = routed + turned[:, 2 + k : 3 + k] * dot(chosen, outs)

    arrived(sdx.at[: T - 1], s_load.at[0], r_sdx.at[0])
    arrived(hsh.at[: T - 1], s_load.at[0], r_hsh.at[0])
    for q in range(T):
        routed = routed + dot_nt(hsh[q], sdx[q].reshape(K * R, C))
    mixed[...] = routed.astype(BF)

    def gone(ref, sem):
        sent(ref, sem.at[0], sem.at[0])

    gone(tk.at[: T - 1], s_tok)
    gone(hsh.at[: T - 1], s_hsh)
    gone(tok, s_raw)
    gone(meta_send, s_meta)
    gone(gu.at[:G], f_gu)
    gone(gu.at[: E - 1], s_gu)
    gone(dn.at[: K // 2], f_dn)
    gone(ret.at[: G - 1], s_ret)
    gone(port.at[:H], p_in)
    gone(hid.at[:H], s_in)
    gone(sh.at[:G], s_shb)
    gone(sdx.at[: T - 1], s_sdx)
    if H > 1:
        gone(port.at[: H - 1], p_out)
        gone(hid.at[: H - 1], s_out)
    if D > 1:
        gone(disp.at[: D - 1], s_da)

        @pl.when(at_gate)
        def _():
            gone(gw_send, s_gw)

    @pl.when(mine)
    def _():
        gone(dn_send.at[: E - 1], s_dn)

    @pl.when(jnp.logical_not(mine))
    def _():
        gone(dn_send, s_dn)

    def done_groups(d):
        @pl.when((d >= g) & (g > 0))
        def _():
            sent(sh.at[f], s_left.at[d], s_left.at[d])

        @pl.when((d <= g) & (g < G - 1))
        def _():
            sent(sh.at[f], s_right.at[d], s_right.at[d])

    loop(0, G, done_groups)


def hand_on(count, *refs):
    copies = [
        pltpu.make_async_copy(refs[i], refs[count + i], refs[-1].at[i])
        for i in range(count)
    ]
    for copy in copies:
        copy.start()
    for copy in copies:
        copy.wait()


def on_device(
    tokens,
    routes,
    route_weight,
    norm_gain,
    expert_gate,
    expert_up,
    expert_down,
    shared_gate,
    shared_up,
    shared_down,
):
    F = lax.axis_size("fs")
    T = lax.axis_size("tp")
    E, R, C = expert_gate.shape
    tok_count, quarter = tokens.shape
    pick_count = routes.shape[1]
    capacity = 2 * ((3 * tok_count * pick_count + 4 * E - 1) // (4 * E))
    slots = (capacity + 15) // 16 * 16
    G, K = F // 2, F // T
    vmem = pl.BlockSpec(memory_space=pltpu.VMEM)
    hbm = pl.BlockSpec(memory_space=pltpu.HBM)
    dma = pltpu.SemaphoreType.DMA
    shapes = [
        (tok_count, quarter),
        (C // 2, F * R),
        (C // 2, F * R),
        (K * R, T * C // 2),
        (F * R, C),
        (F * R, C),
        (C, F * R),
    ]
    H, D, N = T // 2, G // 2, max(R // 64, 1)
    scratch = [
        (T, tok_count, quarter),
        (T, tok_count, quarter),
        (E, R, 2 * C),
        (F, R, 2 * C),
        (E, R, C),
        (K, T, R, C),
        (F, 3, R, C),
        (D, slots, quarter),
        (T, G, slots, quarter),
        (T, G, slots, C),
        (G, slots, quarter),
        (G, slots, quarter),
        (T, tok_count, C),
        (T, K, R, C),
        (D, tok_count, quarter),
        (D, max(D - 1, 1), slots, quarter),
    ]
    wide = [(8, tok_count), (D, 8, tok_count)]
    one = (1,)
    sems = [
        one, (T,), one, (G, N), one, one, one, (K // 2, T), one, one,
        (G,), (G,), one, (G, 3), (G, 2), one, one, one, (H, G), one,
        one, (D,), one, (D,), one, one, one, (H, G), one, one, one, one, one, one,
    ]
    args = (
        tokens,
        routes.T,
        route_weight.T,
        norm_gain[None, :],
        expert_gate,
        expert_up,
        expert_down,
        shared_gate,
        shared_up,
        shared_down,
    )
    results = pl.pallas_call(
        functools.partial(kernel, F, T, slots),
        out_shape=[jax.ShapeDtypeStruct(s, BF) for s in shapes],
        in_specs=[hbm] * 10,
        out_specs=[vmem] * 7,
        scratch_shapes=[pltpu.VMEM(a.shape, a.dtype) for a in args]
        + [dma((len(args),))]
        + [pltpu.VMEM(s, BF) for s in scratch]
        + [pltpu.VMEM(s, F32) for s in wide]
        + [dma(s) for s in sems],
        compiler_params=pltpu.CompilerParams(
            has_side_effects=True, collective_id=0, vmem_limit_bytes=48 * 1024 * 1024
        ),
    )(*[pltpu.with_memory_space_constraint(a, pltpu.HBM) for a in args])
    mixed, gate, up, down, sg, su, sd = pl.pallas_call(
        functools.partial(hand_on, 7),
        out_shape=[jax.ShapeDtypeStruct(s, BF) for s in shapes],
        in_specs=[vmem] * 7,
        out_specs=[hbm] * 7,
        scratch_shapes=[dma((7,))],
        compiler_params=pltpu.CompilerParams(vmem_limit_bytes=8 * 1024 * 1024),
    )(*results)
    return (mixed, gate.T[None], up.T[None], down[None], sg, su, sd)


def solution(mesh):
    in_specs = (
        P("fs", "tp"),
        P("fs", None),
        P("fs", None),
        P("fs"),
        P(None, "fs", "tp"),
        P(None, "fs", "tp"),
        P(None, "fs", "tp"),
        P("fs", "tp"),
        P("fs", "tp"),
        P("tp", "fs"),
    )
    out_specs = (
        P("fs", "tp"),
        P("fs", None, "tp"),
        P("fs", None, "tp"),
        P("fs", "tp", None),
        P(None, "tp"),
        P(None, "tp"),
        P("tp", None),
    )
    return jax.shard_map(
        on_device, mesh=mesh, in_specs=in_specs, out_specs=out_specs, check_vma=False
    )
```

```python
import functools

import jax
import jax.numpy as jnp
from jax import lax
from jax.experimental import pallas as pl
from jax.experimental.pallas import tpu as pltpu
from jax.sharding import PartitionSpec as P

EPS = 1e-06
BF = jnp.bfloat16
F32 = jnp.float32


def loop(low, high, body):
    def step(i, carry):
        body(i)
        return carry

    lax.fori_loop(low, high, step, 0)


def dot(a, b):
    return jnp.dot(a, b, preferred_element_type=F32)


def dot_nt(a, b):
    return lax.dot_general(a, b, (((1,), (1,)), ((), ())), preferred_element_type=F32)


def left_halves(a, b, half):
    lane = lax.broadcasted_iota(jnp.int32, a.shape, 1)
    return jnp.where(lane < half, a, pltpu.roll(b, half, 1))


def right_halves(a, b, half):
    lane = lax.broadcasted_iota(jnp.int32, a.shape, 1)
    return jnp.where(lane < half, pltpu.roll(a, half, 1), b)


def silu(v):
    return v / (1.0 + jnp.exp(-v))


def kernel(
    F,
    T,
    slots,
    tok_in,
    routes_in,
    weight_in,
    gain_in,
    eg_in,
    eu_in,
    ed_in,
    sg_in,
    su_in,
    sd_in,
    mixed,
    gate_out,
    up_out,
    dn_out,
    sg_out,
    su_out,
    sd_out,
    tok,
    routes,
    weight,
    gain,
    eg,
    eu,
    ed,
    sg,
    su,
    sd,
    s_load,
    tk,
    nm,
    gu_send,
    gu,
    dn_send,
    dn,
    sh,
    disp,
    port,
    hid,
    ret_send,
    ret,
    hsh,
    sdx,
    raw,
    gw_send,
    meta_send,
    meta,
    s_tok,
    r_tok,
    s_gu,
    r_gu,
    x_gu,
    f_gu,
    s_dn,
    r_dn,
    x_dn,
    f_dn,
    s_left,
    s_right,
    s_shb,
    r_sh,
    r_shp,
    s_da,
    p_out,
    p_in,
    r_port,
    x_port,
    s_raw,
    r_raw,
    s_meta,
    r_meta,
    s_gw,
    s_out,
    s_in,
    r_hid,
    s_ret,
    r_ret,
    s_hsh,
    r_hsh,
    s_sdx,
    r_sdx,
):
    G = F // 2
    K = F // T
    H = T // 2
    E = eg.shape[0]
    R, C = eg.shape[1], eg.shape[2]
    half = C // 2
    tok_count = tok.shape[0]
    quarter = tok.shape[1]
    width = quarter * T
    f = lax.axis_index("fs")
    t = lax.axis_index("tp")
    g, p = f // 2, f % 2
    pair = g * 2 + (1 - p)
    y, c = t // 2, t % 2
    t_pair = y * 2 + (1 - c)
    home = f // K
    pieces = r_gu.shape[1]
    D = G // 2
    step = R // pieces
    mine = home == t

    def far_first(i):
        return jnp.where(2 * g < G, G - 1 - i, i)

    def near_first(i):
        return jnp.where(2 * g < G, i, G - 1 - i)

    def send_order(i):
        return jnp.where(i < G // 2, near_first(i), far_first(i - G // 2))

    left = 2 * g < G
    depth = jnp.where(left, g, G - 1 - g)
    gateway = jnp.where(left, D, D - 1)

    def remote(src, dst, send, recv, fs, tp):
        return pltpu.make_async_remote_copy(
            src_ref=src,
            dst_ref=dst,
            send_sem=send,
            recv_sem=recv,
            device_id={"fs": fs, "tp": tp},
            device_id_type=pl.DeviceIdType.MESH,
        )

    def arrived(dst, send, recv):
        remote(dst, dst, send, recv, pair, t).wait_recv()

    def sent(src, send, recv):
        remote(src, src, send, recv, pair, t).wait_send()

    loads = [
        pltpu.make_async_copy(src, dst, s_load.at[i])
        for i, (src, dst) in enumerate(
            (
                (tok_in, tok),
                (routes_in, routes),
                (weight_in, weight),
                (gain_in, gain),
                (eg_in, eg),
                (eu_in, eu),
                (ed_in, ed),
                (sg_in, sg),
                (su_in, su),
                (sd_in, sd),
            )
        )
    ]
    for load in loads:
        load.start()

    barrier = pltpu.get_barrier_semaphore()

    def greet(fs, tp):
        pl.semaphore_signal(
            barrier,
            inc=1,
            device_id={"fs": fs, "tp": tp},
            device_id_type=pl.DeviceIdType.MESH,
        )

    loop(1, G, lambda d: greet(2 * ((g + d) % G) + p, t))
    greet(pair, t)
    loop(1, T, lambda d: greet(f, (t + d) % T))

    def greet_rows(i):
        row = t * K + 2 * i + p

        @pl.when(row != f)
        def _():
            loop(1, T, lambda d: greet(row, (t + d) % T))

    loop(0, K // 2, greet_rows)

    for load in loads[:2]:
        load.wait()
    named_by = routes[...].astype(F32)
    line = lax.broadcasted_iota(jnp.int32, (8, tok_count), 0)
    meta_send[...] = jnp.where(line == 0, named_by[0:1], named_by[1:2])
    rows = lax.broadcasted_iota(jnp.int32, (tok_count, tok_count), 0)
    cols = lax.broadcasted_iota(jnp.int32, (tok_count, tok_count), 1)
    after = (rows < cols).astype(F32).astype(BF)
    slot_rows = lax.broadcasted_iota(jnp.int32, (slots, tok_count), 0)

    def pack(e, names, block):
        chosen = e.astype(F32)
        held = ((names[0:1] == chosen) | (names[1:2] == chosen)).astype(F32)
        spots = dot(jnp.broadcast_to(held, (16, tok_count)).astype(BF), after)
        here = (slot_rows == spots[0:1].astype(jnp.int32)) & (held > 0.5)
        return dot(here.astype(F32).astype(BF), block).astype(BF)

    def at_depth(i):
        return jnp.where(left, i, G - 1 - i)

    for i in range(D):
        disp[i] = pack(at_depth(i), meta_send[...], tok[...])
    pl.semaphore_wait(barrier, G + T - 1 + (G - 1) * jnp.where(mine, 0, 1))
    remote(tok, raw.at[depth], s_raw.at[0], r_raw.at[depth], 2 * gateway + p, t).start()
    remote(
        meta_send, meta.at[depth], s_meta.at[0], r_meta.at[depth], 2 * gateway + p, t
    ).start()

    def send_disp(i):
        @pl.when(i != depth)
        def _():
            remote(
                disp.at[i],
                port.at[t, g],
                s_da.at[0],
                r_port.at[0, g],
                2 * at_depth(i) + p,
                t,
            ).start()

    loop(0, D, send_disp)
    port[t, g] = disp[depth]

    def port_copy(src, group, sem, recv, to):
        return remote(port.at[src, group], port.at[src, group], sem, recv, f, to)

    def pass_block(group):
        for o in range(1, H):
            port_copy(
                t, group, p_out.at[0], r_port.at[H - o, group], (t + 2 * o) % T
            ).start()
        port_copy(t, group, p_in.at[0], x_port.at[0], t_pair).start()

    pass_block(g)

    def tok_copy(src, sem, to):
        return remote(tk.at[src], tk.at[src], sem, r_tok.at[src], f, to)

    for o in range(1, H):
        remote(tok, tk.at[t], s_tok.at[0], r_tok.at[t], f, (t + 2 * o) % T).start()
    remote(tok, tk.at[t], s_tok.at[0], r_tok.at[t], f, t_pair).start()
    tk[t] = tok[...]

    def shared_copy(block, i, sems, recv, to):
        return remote(sh.at[block, i], sh.at[block, i], sems, recv, to, t)

    def share_left(block, i):
        @pl.when(g > 0)
        def _():
            shared_copy(block, i, s_left.at[block // 2], r_sh.at[block // 2, i], f - 2).start()

    def share_right(block, i):
        @pl.when(g < G - 1)
        def _():
            shared_copy(block, i, s_right.at[block // 2], r_sh.at[block // 2, i], f + 2).start()

    def share_pair(block, i):
        shared_copy(block, i, s_shb.at[0], r_shp.at[block // 2, (i + 1) // 2], pair).start()

    def spread(block):
        @pl.when(block // K != t)
        def _():
            remote(
                sh.at[block, 0],
                sdx.at[t, block % K],
                s_sdx.at[0],
                r_sdx.at[0],
                f,
                block // K,
            ).start()

    def relay_right(k, low, high, across):
        @pl.when(g - k >= 0)
        def _():
            block = f - 2 * k

            def piece(i):
                arrived(sh.at[block, i], s_load.at[0], r_sh.at[block // 2, i])
                share_right(block, i)
                if across:
                    share_pair(block, i)

            loop(low, high, piece)
            if low == 0:
                spread(block)

    def relay_left(k, low, high, across):
        @pl.when(g + k < G)
        def _():
            block = f + 2 * k

            def piece(i):
                arrived(sh.at[block, i], s_load.at[0], r_sh.at[block // 2, i])
                share_left(block, i)
                if across:
                    share_pair(block, i)

            loop(low, high, piece)
            if low == 0:
                spread(block)

    def over_right(k):
        @pl.when(g - k >= 0)
        def _():
            loop(0, 3, lambda i: share_pair(f - 2 * k, i))

    def over_left(k):
        @pl.when(g + k < G)
        def _():
            loop(0, 3, lambda i: share_pair(f + 2 * k, i))

    def relay_in(k, low=0, high=3, across=False):
        @pl.when(left)
        def _():
            relay_right(k, low, high, across)

        @pl.when(jnp.logical_not(left))
        def _():
            relay_left(k, low, high, across)

    def relay_out(k, low=0, high=3, across=False):
        @pl.when(left)
        def _():
            relay_left(k, low, high, across)

        @pl.when(jnp.logical_not(left))
        def _():
            relay_right(k, low, high, across)

    def over_in(k):
        @pl.when(left)
        def _():
            over_right(k)

        @pl.when(jnp.logical_not(left))
        def _():
            over_left(k)

    def over_out(k):
        @pl.when(left)
        def _():
            over_left(k)

        @pl.when(jnp.logical_not(left))
        def _():
            over_right(k)

    for load in loads[2:6]:
        load.wait()
    gains = jnp.broadcast_to(gain[...], (8, R)).T[:, 0:1]

    def rows_of(n):
        return pl.ds(pl.multiple_of(n * step, step), step)

    def send_gu(i):
        e = send_order(i)
        gu_send[e, :, :C] = (eg[e] * gains).astype(BF)
        gu_send[e, :, C:] = (eu[e] * gains).astype(BF)

        @pl.when(e != g)
        def _():
            def piece(n):
                remote(
                    gu_send.at[e, rows_of(n)],
                    gu.at[f, rows_of(n)],
                    s_gu.at[0],
                    r_gu.at[g, n],
                    2 * e + p,
                    t,
                ).start()

            loop(0, pieces, piece)

    loop(0, D, send_gu)
    gu[f] = gu_send[g]

    for load in loads[6:]:
        load.wait()
    sh[f, 0] = sd[...].T.astype(BF)
    sh[f, 1] = (sg[...] * gains).astype(BF)
    sh[f, 2] = (su[...] * gains).astype(BF)
    spread(f)
    at_end = (g == 0) | (g == G - 1)

    @pl.when(at_end)
    def _():
        loop(0, 3, lambda i: share_left(f, i))
        loop(0, 3, lambda i: share_right(f, i))

    loop(D, E, send_gu)

    def cross(src, n):
        remote(
            gu.at[src, rows_of(n)],
            gu.at[src, rows_of(n)],
            f_gu.at[0],
            x_gu.at[0],
            pair,
            t,
        ).start()

    loop(0, pieces, lambda n: cross(f, n))

    loop(0, 3, lambda i: share_pair(f, i))

    def take_block(group):
        arrived(port.at[t, group], s_load.at[0], r_port.at[0, group])
        pass_block(group)

    def take_side(i):
        @pl.when(i != depth)
        def _():
            take_block(at_depth(i))

    def take_other(i):
        take_block(at_depth(G - 1 - i))

    def open_block(i):
        group = at_depth(G - 1 - i)
        arrived(raw.at[i], s_load.at[0], r_raw.at[i])
        arrived(meta.at[i], s_load.at[0], r_meta.at[i])
        for k in range(D - 1):
            gw_send[i, k] = pack(at_depth(k), meta[i], raw[i])
            remote(
                gw_send.at[i, k],
                port.at[t, group],
                s_gw.at[0],
                r_port.at[0, group],
                2 * at_depth(k) + p,
                t,
            ).start()
        port[t, group] = pack(g, meta[i], raw[i])
        pass_block(group)

    def inner_block(i):
        group = near_first(i)
        for o in range(1, H):
            src = (t + 2 * o) % T
            arrived(port.at[src, group], s_load.at[0], r_port.at[o, group])
            port_copy(src, group, p_in.at[0], x_port.at[0], t_pair).start()


    def take_near(i):
        src = 2 * jnp.where(2 * g < G, i, G - 1 - i) + p

        @pl.when(src != f)
        def _():
            def piece(n):
                arrived(gu.at[src, rows_of(n)], s_load.at[0], r_gu.at[src // 2, n])
                cross(src, n)

            loop(0, pieces, piece)


    def take_far(n):
        def block(i):
            src = 2 * jnp.where(2 * g < G, G // 2 + i, G // 2 - 1 - i) + p
            arrived(gu.at[src, rows_of(n)], s_load.at[0], r_gu.at[src // 2, n])
            cross(src, n)

        loop(0, G // 2, block)


    def expert_hidden(i):
        group = near_first(i)
        total = jnp.zeros((slots, 2 * C), F32)
        squares = jnp.zeros((slots, 1), F32)
        for q in range(T):
            total = total + dot(
                port[q, group], gu[q * K : (q + 1) * K].reshape(quarter, 2 * C)
            )
            x = port[q, group].astype(F32)
            squares = squares + jnp.sum(x * x, axis=1, keepdims=True)
        total = total * lax.rsqrt(squares / width + EPS)
        hid[t, group] = (silu(total[:, :C]) * total[:, C:]).astype(BF)
        for o in range(1, H):
            remote(
                hid.at[t, group],
                hid.at[t, group],
                s_out.at[0],
                r_hid.at[H - o, group],
                f,
                (t + 2 * o) % T,
            ).start()
        remote(
            hid.at[t, group],
            hid.at[t, group],
            s_in.at[0],
            r_hid.at[0, group],
            f,
            t_pair,
        ).start()


    def pass_hidden(i):
        group = near_first(i)
        for o in range(1, H):
            src = (t + 2 * o) % T
            arrived(hid.at[src, group], s_load.at[0], r_hid.at[o, group])
            remote(
                hid.at[src, group],
                hid.at[src, group],
                s_in.at[0],
                r_hid.at[0, group],
                f,
                t_pair,
            ).start()


    def send_ret(group):
        remote(
            ret_send.at[group], ret.at[g], s_ret.at[0], r_ret.at[0], 2 * group + p, t
        ).start()

    def expert_out(i):
        group = near_first(i)
        arrived(hid.at[:H, group], s_load.at[0], r_hid.at[0, group])
        total = jnp.zeros((slots, quarter), F32)
        for q in range(T):
            total = total + dot_nt(hid[q, group], dn[:, q].reshape(K * R, C))
        ret_send[group] = total.astype(BF)

        @pl.when((group != g) & (i < G - 1))
        def _():
            send_ret(group)


    at_gate = depth == D - 1

    @pl.when(at_gate)
    def _():
        loop(0, D, lambda i: open_block(D - 1 - i))

    loop(0, D, take_side)

    def send_dn(i):
        e = send_order(i)
        dn_send[e] = ed[e].astype(BF)

        @pl.when(jnp.logical_not((e == g) & mine))
        def _():
            remote(
                dn_send.at[e], dn.at[f % K, t], s_dn.at[0], r_dn.at[f % K // 2, t], 2 * e + p, home
            ).start()

    loop(0, E, send_dn)

    @pl.when(mine)
    def _():
        dn[f % K, t] = dn_send[g]

    @pl.when(jnp.logical_not(at_end))
    def _():
        loop(0, 3, lambda i: share_left(f, i))
        loop(0, 3, lambda i: share_right(f, i))


    def hand_across(i):
        k = 2 * i + p

        def chunk(q):
            @pl.when(jnp.logical_not((t * K + k == f) & (q == t)))
            def _():
                arrived(dn.at[k, q], s_load.at[0], r_dn.at[i, q])

            remote(dn.at[k, q], dn.at[k, q], f_dn.at[0], x_dn.at[0], pair, t).start()

        loop(0, T, chunk)

    loop(0, G // 2, take_near)
    loop(1, G // 2, relay_in)
    loop(1, G // 2, over_in)
    loop(0, pieces // 2, take_far)

    @pl.when(jnp.logical_not(at_gate))
    def _():
        loop(0, D, lambda i: take_other(D - 1 - i))

    loop(pieces // 2, pieces, take_far)
    @pl.when(at_end)
    def _():
        loop(0, K // 2, hand_across)

    loop(0, G, inner_block)
    @pl.when(jnp.logical_not(at_end))
    def _():
        loop(0, K // 2, hand_across)


    for o in range(1, H):
        src = (t + 2 * o) % T
        arrived(tk.at[src], s_load.at[0], r_tok.at[src])
        tok_copy(src, s_tok.at[0], t_pair).start()
    for o in range(H):
        src = (t_pair + 2 * o) % T
        arrived(tk.at[src], s_load.at[0], r_tok.at[src])
    squares = jnp.zeros((tok_count, 1), F32)
    for q in range(T):
        x = tk[q].astype(F32)
        squares = squares + jnp.sum(x * x, axis=1, keepdims=True)
    scale = lax.rsqrt(squares / width + EPS)
    for q in range(T):
        nm[q] = (tk[q].astype(F32) * scale).astype(BF)
    arrived(port.at[:H], s_load.at[0], x_port.at[0])
    arrived(gu.at[:G], s_load.at[0], x_gu.at[0])
    loop(0, G, expert_hidden)
    loop(1, min(2, G), lambda k: relay_out(k, across=True))
    loop(0, G, pass_hidden)
    @pl.when(jnp.logical_not(at_end))
    def _():
        loop(2, G // 2 + 1, relay_out)
        loop(2, G // 2 + 1, over_out)

    @pl.when(at_end)
    def _():
        loop(2, G // 2 + 1, lambda k: relay_out(k, across=True))

    arrived(dn.at[: K // 2], s_load.at[0], x_dn.at[0])
    loop(0, G, expert_out)
    ret[g] = ret_send[g]


    def late_out(k):
        relay_out(k, across=True)

    def late_in(k):
        relay_in(k, across=True)

    loop(G // 2 + 1, G, late_out)
    loop(G // 2, G, late_in)

    def place_down(k):
        for q in range(0, T, 2):
            a, b = dn[k, q].astype(F32), dn[k, q + 1].astype(F32)
            block = jnp.where(
                p == 0, left_halves(a, b, half), right_halves(a, b, half)
            )
            dn_out[pl.ds(pl.multiple_of(k * R, R), R), q * half : (q + 2) * half] = block.astype(BF)

    loop(0, K, place_down)

    def wait_down(i):
        block = near_first(i) * 2 + 1 - p
        arrived(sh.at[block, 0], s_load.at[0], r_shp.at[block // 2, 0])
        spread(block)
        arrived(sh.at[block, 1:3], s_load.at[0], r_shp.at[block // 2, 1])

    send_ret(near_first(G - 1))
    loop(0, G, wait_down)

    gate_sh = sh[:, 1].reshape(F * R, C)
    up_sh = sh[:, 2].reshape(F * R, C)
    act = jnp.zeros((tok_count, C), F32)
    lin = jnp.zeros((tok_count, C), F32)
    for q in range(T):
        act = act + dot(nm[q], gate_sh[q * quarter : (q + 1) * quarter])
        lin = lin + dot(nm[q], up_sh[q * quarter : (q + 1) * quarter])
    hsh[t] = (silu(act) * lin).astype(BF)

    def send_hsh(d):
        remote(
            hsh.at[t], hsh.at[t], s_hsh.at[0], r_hsh.at[0], f, (t + d) % T
        ).start()

    loop(1, T, send_hsh)

    def keep_down(k):
        sdx[t, k] = sh[t * K + k, 0]

    loop(0, K, keep_down)

    for q in range(T):
        span = slice(q * quarter, (q + 1) * quarter)
        sd_out[:, span] = (
            sh[q * K : (q + 1) * K, 0].reshape(quarter, C).astype(F32).T.astype(BF)
        )
    sg_out[...] = sh[:, 1].reshape(F * R, C)
    su_out[...] = sh[:, 2].reshape(F * R, C)

    for q in range(T):
        span = slice(q * quarter, (q + 1) * quarter)
        whole = gu[q * K : (q + 1) * K].reshape(quarter, 2 * C).astype(F32)
        gate, up = whole[:, :C].T, whole[:, C:].T
        gate_out[:, span] = jnp.where(p == 0, gate[:half], gate[half:]).astype(BF)
        up_out[:, span] = jnp.where(p == 0, up[:half], up[half:]).astype(BF)

    experts = lax.broadcasted_iota(jnp.int32, (tok_count, E), 1)
    turned = jnp.where(line == 2, weight[0:1, :], meta_send[...])
    turned = jnp.where(line == 3, weight[1:2, :], turned).T
    first, second = turned[:, 0:1].astype(jnp.int32), turned[:, 1:2].astype(jnp.int32)
    named = ((experts == first) | (experts == second)).astype(F32)
    before = (cols < rows).astype(F32).astype(BF)
    place = dot(before, named.astype(BF))
    slot_ids = lax.broadcasted_iota(jnp.int32, (tok_count, E * slots), 1)

    def pick_of(chosen):
        spot = jnp.sum(jnp.where(experts == chosen, place, 0.0), axis=1, keepdims=True)
        return slot_ids == chosen * slots + spot.astype(jnp.int32)

    pick0, pick1 = pick_of(first), pick_of(second)

    arrived(ret.at[: G - 1], s_load.at[0], r_ret.at[0])
    outs = ret[...].reshape(E * slots, quarter)
    routed = jnp.zeros((tok_count, quarter), F32)
    for k, pick in enumerate((pick0, pick1)):
        chosen = jnp.where(pick, 1.0, 0.0).astype(BF)
        routed = routed + turned[:, 2 + k : 3 + k] * dot(chosen, outs)

    arrived(sdx.at[: T - 1], s_load.at[0], r_sdx.at[0])
    arrived(hsh.at[: T - 1], s_load.at[0], r_hsh.at[0])
    for q in range(T):
        routed = routed + dot_nt(hsh[q], sdx[q].reshape(K * R, C))
    mixed[...] = routed.astype(BF)

    def gone(ref, sem):
        sent(ref, sem.at[0], sem.at[0])

    gone(tk.at[: T - 1], s_tok)
    gone(hsh.at[: T - 1], s_hsh)
    gone(tok, s_raw)
    gone(meta_send, s_meta)
    gone(gu.at[:G], f_gu)
    gone(gu.at[: E - 1], s_gu)
    gone(dn.at[: K // 2], f_dn)
    gone(ret.at[: G - 1], s_ret)
    gone(port.at[:H], p_in)
    gone(hid.at[:H], s_in)
    gone(sh.at[:G], s_shb)
    gone(sdx.at[: T - 1], s_sdx)
    if H > 1:
        gone(port.at[: H - 1], p_out)
        gone(hid.at[: H - 1], s_out)
    if D > 1:
        gone(disp.at[: D - 1], s_da)

        @pl.when(at_gate)
        def _():
            gone(gw_send, s_gw)

    @pl.when(mine)
    def _():
        gone(dn_send.at[: E - 1], s_dn)

    @pl.when(jnp.logical_not(mine))
    def _():
        gone(dn_send, s_dn)

    def done_groups(d):
        @pl.when((d >= g) & (g > 0))
        def _():
            sent(sh.at[f], s_left.at[d], s_left.at[d])

        @pl.when((d <= g) & (g < G - 1))
        def _():
            sent(sh.at[f], s_right.at[d], s_right.at[d])

    loop(0, G, done_groups)


def hand_on(count, *refs):
    copies = [
        pltpu.make_async_copy(refs[i], refs[count + i], refs[-1].at[i])
        for i in range(count)
    ]
    for copy in copies:
        copy.start()
    for copy in copies:
        copy.wait()


def on_device(
    tokens,
    routes,
    route_weight,
    norm_gain,
    expert_gate,
    expert_up,
    expert_down,
    shared_gate,
    shared_up,
    shared_down,
):
    F = lax.axis_size("fs")
    T = lax.axis_size("tp")
    E, R, C = expert_gate.shape
    tok_count, quarter = tokens.shape
    pick_count = routes.shape[1]
    capacity = 2 * ((3 * tok_count * pick_count + 4 * E - 1) // (4 * E))
    slots = (capacity + 15) // 16 * 16
    G, K = F // 2, F // T
    vmem = pl.BlockSpec(memory_space=pltpu.VMEM)
    hbm = pl.BlockSpec(memory_space=pltpu.HBM)
    dma = pltpu.SemaphoreType.DMA
    shapes = [
        (tok_count, quarter),
        (C // 2, F * R),
        (C // 2, F * R),
        (K * R, T * C // 2),
        (F * R, C),
        (F * R, C),
        (C, F * R),
    ]
    H, D, N = T // 2, G // 2, max(R // 64, 1)
    scratch = [
        (T, tok_count, quarter),
        (T, tok_count, quarter),
        (E, R, 2 * C),
        (F, R, 2 * C),
        (E, R, C),
        (K, T, R, C),
        (F, 3, R, C),
        (D, slots, quarter),
        (T, G, slots, quarter),
        (T, G, slots, C),
        (G, slots, quarter),
        (G, slots, quarter),
        (T, tok_count, C),
        (T, K, R, C),
        (D, tok_count, quarter),
        (D, max(D - 1, 1), slots, quarter),
    ]
    wide = [(8, tok_count), (D, 8, tok_count)]
    one = (1,)
    sems = [
        one, (T,), one, (G, N), one, one, one, (K // 2, T), one, one,
        (G,), (G,), one, (G, 3), (G, 2), one, one, one, (H, G), one,
        one, (D,), one, (D,), one, one, one, (H, G), one, one, one, one, one, one,
    ]
    args = (
        tokens,
        routes.T,
        route_weight.T,
        norm_gain[None, :],
        expert_gate,
        expert_up,
        expert_down,
        shared_gate,
        shared_up,
        shared_down,
    )
    results = pl.pallas_call(
        functools.partial(kernel, F, T, slots),
        out_shape=[jax.ShapeDtypeStruct(s, BF) for s in shapes],
        in_specs=[hbm] * 10,
        out_specs=[vmem] * 7,
        scratch_shapes=[pltpu.VMEM(a.shape, a.dtype) for a in args]
        + [dma((len(args),))]
        + [pltpu.VMEM(s, BF) for s in scratch]
        + [pltpu.VMEM(s, F32) for s in wide]
        + [dma(s) for s in sems],
        compiler_params=pltpu.CompilerParams(
            has_side_effects=True, collective_id=0, vmem_limit_bytes=48 * 1024 * 1024
        ),
    )(*[pltpu.with_memory_space_constraint(a, pltpu.HBM) for a in args])
    mixed, gate, up, down, sg, su, sd = pl.pallas_call(
        functools.partial(hand_on, 7),
        out_shape=[jax.ShapeDtypeStruct(s, BF) for s in shapes],
        in_specs=[vmem] * 7,
        out_specs=[hbm] * 7,
        scratch_shapes=[dma((7,))],
        compiler_params=pltpu.CompilerParams(vmem_limit_bytes=8 * 1024 * 1024),
    )(*results)
    return (mixed, gate.T[None], up.T[None], down[None], sg, su, sd)


def solution(mesh):
    in_specs = (
        P("fs", "tp"),
        P("fs", None),
        P("fs", None),
        P("fs"),
        P(None, "fs", "tp"),
        P(None, "fs", "tp"),
        P(None, "fs", "tp"),
        P("fs", "tp"),
        P("fs", "tp"),
        P("tp", "fs"),
    )
    out_specs = (
        P("fs", "tp"),
        P("fs", None, "tp"),
        P("fs", None, "tp"),
        P("fs", "tp", None),
        P(None, "tp"),
        P(None, "tp"),
        P("tp", None),
    )
    return jax.shard_map(
        on_device, mesh=mesh, in_specs=in_specs, out_specs=out_specs, check_vma=False
    )
```

```python
import functools

import jax
import jax.numpy as jnp
from jax import lax
from jax.experimental import pallas as pl
from jax.experimental.pallas import tpu as pltpu
from jax.sharding import PartitionSpec as P

EPS = 1e-06
BF = jnp.bfloat16
F32 = jnp.float32


def loop(low, high, body):
    def step(i, carry):
        body(i)
        return carry

    lax.fori_loop(low, high, step, 0)


def dot(a, b):
    return jnp.dot(a, b, preferred_element_type=F32)


def dot_nt(a, b):
    return lax.dot_general(a, b, (((1,), (1,)), ((), ())), preferred_element_type=F32)


def left_halves(a, b, half):
    lane = lax.broadcasted_iota(jnp.int32, a.shape, 1)
    return jnp.where(lane < half, a, pltpu.roll(b, half, 1))


def right_halves(a, b, half):
    lane = lax.broadcasted_iota(jnp.int32, a.shape, 1)
    return jnp.where(lane < half, pltpu.roll(a, half, 1), b)


def silu(v):
    return v / (1.0 + jnp.exp(-v))


def kernel(
    F,
    T,
    slots,
    tok_in,
    routes_in,
    weight_in,
    gain_in,
    eg_in,
    eu_in,
    ed_in,
    sg_in,
    su_in,
    sd_in,
    mixed,
    gate_out,
    up_out,
    dn_out,
    sg_out,
    su_out,
    sd_out,
    tok,
    routes,
    weight,
    gain,
    eg,
    eu,
    ed,
    sg,
    su,
    sd,
    s_load,
    tk,
    nm,
    gu_send,
    gu,
    dn_send,
    dn,
    sh,
    disp,
    port,
    hid,
    ret_send,
    ret,
    hsh,
    sdx,
    raw,
    gw_send,
    meta_send,
    meta,
    s_tok,
    r_tok,
    s_gu,
    r_gu,
    x_gu,
    f_gu,
    s_dn,
    r_dn,
    x_dn,
    f_dn,
    s_left,
    s_right,
    s_shb,
    r_sh,
    r_shp,
    s_da,
    p_out,
    p_in,
    r_port,
    x_port,
    s_raw,
    r_raw,
    s_meta,
    r_meta,
    s_gw,
    s_out,
    s_in,
    r_hid,
    s_ret,
    r_ret,
    s_hsh,
    r_hsh,
    s_sdx,
    r_sdx,
):
    G = F // 2
    K = F // T
    H = T // 2
    E = eg.shape[0]
    R, C = eg.shape[1], eg.shape[2]
    half = C // 2
    tok_count = tok.shape[0]
    quarter = tok.shape[1]
    width = quarter * T
    f = lax.axis_index("fs")
    t = lax.axis_index("tp")
    g, p = f // 2, f % 2
    pair = g * 2 + (1 - p)
    y, c = t // 2, t % 2
    t_pair = y * 2 + (1 - c)
    home = f // K
    pieces = r_gu.shape[1]
    D = G // 2
    step = R // pieces
    mine = home == t

    def far_first(i):
        return jnp.where(2 * g < G, G - 1 - i, i)

    def near_first(i):
        return jnp.where(2 * g < G, i, G - 1 - i)

    def send_order(i):
        return jnp.where(i < G // 2, near_first(i), far_first(i - G // 2))

    left = 2 * g < G
    depth = jnp.where(left, g, G - 1 - g)
    gateway = jnp.where(left, D, D - 1)

    def remote(src, dst, send, recv, fs, tp):
        return pltpu.make_async_remote_copy(
            src_ref=src,
            dst_ref=dst,
            send_sem=send,
            recv_sem=recv,
            device_id={"fs": fs, "tp": tp},
            device_id_type=pl.DeviceIdType.MESH,
        )

    def arrived(dst, send, recv):
        remote(dst, dst, send, recv, pair, t).wait_recv()

    def sent(src, send, recv):
        remote(src, src, send, recv, pair, t).wait_send()

    loads = [
        pltpu.make_async_copy(src, dst, s_load.at[i])
        for i, (src, dst) in enumerate(
            (
                (tok_in, tok),
                (routes_in, routes),
                (weight_in, weight),
                (gain_in, gain),
                (eg_in, eg),
                (eu_in, eu),
                (ed_in, ed),
                (sg_in, sg),
                (su_in, su),
                (sd_in, sd),
            )
        )
    ]
    for load in loads:
        load.start()

    barrier = pltpu.get_barrier_semaphore()

    def greet(fs, tp):
        pl.semaphore_signal(
            barrier,
            inc=1,
            device_id={"fs": fs, "tp": tp},
            device_id_type=pl.DeviceIdType.MESH,
        )

    loop(1, G, lambda d: greet(2 * ((g + d) % G) + p, t))
    greet(pair, t)
    loop(1, T, lambda d: greet(f, (t + d) % T))

    def greet_rows(i):
        row = t * K + 2 * i + p

        @pl.when(row != f)
        def _():
            loop(1, T, lambda d: greet(row, (t + d) % T))

    loop(0, K // 2, greet_rows)

    for load in loads[:2]:
        load.wait()
    named_by = routes[...].astype(F32)
    line = lax.broadcasted_iota(jnp.int32, (8, tok_count), 0)
    meta_send[...] = jnp.where(line == 0, named_by[0:1], named_by[1:2])
    rows = lax.broadcasted_iota(jnp.int32, (tok_count, tok_count), 0)
    cols = lax.broadcasted_iota(jnp.int32, (tok_count, tok_count), 1)
    after = (rows < cols).astype(F32).astype(BF)
    slot_rows = lax.broadcasted_iota(jnp.int32, (slots, tok_count), 0)

    def pack(e, names, block):
        chosen = e.astype(F32)
        held = ((names[0:1] == chosen) | (names[1:2] == chosen)).astype(F32)
        spots = dot(jnp.broadcast_to(held, (16, tok_count)).astype(BF), after)
        here = (slot_rows == spots[0:1].astype(jnp.int32)) & (held > 0.5)
        return dot(here.astype(F32).astype(BF), block).astype(BF)

    def at_depth(i):
        return jnp.where(left, i, G - 1 - i)

    for i in range(D):
        disp[i] = pack(at_depth(i), meta_send[...], tok[...])
    pl.semaphore_wait(barrier, G + T - 1 + (G - 1) * jnp.where(mine, 0, 1))
    remote(tok, raw.at[depth], s_raw.at[0], r_raw.at[depth], 2 * gateway + p, t).start()
    remote(
        meta_send, meta.at[depth], s_meta.at[0], r_meta.at[depth], 2 * gateway + p, t
    ).start()

    def send_disp(i):
        @pl.when(i != depth)
        def _():
            remote(
                disp.at[i],
                port.at[t, g],
                s_da.at[0],
                r_port.at[0, g],
                2 * at_depth(i) + p,
                t,
            ).start()

    loop(0, D, send_disp)
    port[t, g] = disp[depth]

    def port_copy(src, group, sem, recv, to):
        return remote(port.at[src, group], port.at[src, group], sem, recv, f, to)

    def pass_block(group):
        for o in range(1, H):
            port_copy(
                t, group, p_out.at[0], r_port.at[H - o, group], (t + 2 * o) % T
            ).start()
        port_copy(t, group, p_in.at[0], x_port.at[0], t_pair).start()

    pass_block(g)

    def tok_copy(src, sem, to):
        return remote(tk.at[src], tk.at[src], sem, r_tok.at[src], f, to)

    for o in range(1, H):
        remote(tok, tk.at[t], s_tok.at[0], r_tok.at[t], f, (t + 2 * o) % T).start()
    remote(tok, tk.at[t], s_tok.at[0], r_tok.at[t], f, t_pair).start()
    tk[t] = tok[...]

    def shared_copy(block, i, sems, recv, to):
        return remote(sh.at[block, i], sh.at[block, i], sems, recv, to, t)

    def share_left(block, i):
        @pl.when(g > 0)
        def _():
            shared_copy(block, i, s_left.at[block // 2], r_sh.at[block // 2, i], f - 2).start()

    def share_right(block, i):
        @pl.when(g < G - 1)
        def _():
            shared_copy(block, i, s_right.at[block // 2], r_sh.at[block // 2, i], f + 2).start()

    def share_pair(block, i):
        shared_copy(block, i, s_shb.at[0], r_shp.at[block // 2, (i + 1) // 2], pair).start()

    def spread(block):
        @pl.when(block // K != t)
        def _():
            remote(
                sh.at[block, 0],
                sdx.at[t, block % K],
                s_sdx.at[0],
                r_sdx.at[0],
                f,
                block // K,
            ).start()

    def relay_right(k, low, high, across):
        @pl.when(g - k >= 0)
        def _():
            block = f - 2 * k

            def piece(i):
                arrived(sh.at[block, i], s_load.at[0], r_sh.at[block // 2, i])
                share_right(block, i)
                if across:
                    share_pair(block, i)

            loop(low, high, piece)
            if low == 0:
                spread(block)

    def relay_left(k, low, high, across):
        @pl.when(g + k < G)
        def _():
            block = f + 2 * k

            def piece(i):
                arrived(sh.at[block, i], s_load.at[0], r_sh.at[block // 2, i])
                share_left(block, i)
                if across:
                    share_pair(block, i)

            loop(low, high, piece)
            if low == 0:
                spread(block)

    def over_right(k):
        @pl.when(g - k >= 0)
        def _():
            loop(0, 3, lambda i: share_pair(f - 2 * k, i))

    def over_left(k):
        @pl.when(g + k < G)
        def _():
            loop(0, 3, lambda i: share_pair(f + 2 * k, i))

    def relay_in(k, low=0, high=3, across=False):
        @pl.when(left)
        def _():
            relay_right(k, low, high, across)

        @pl.when(jnp.logical_not(left))
        def _():
            relay_left(k, low, high, across)

    def relay_out(k, low=0, high=3, across=False):
        @pl.when(left)
        def _():
            relay_left(k, low, high, across)

        @pl.when(jnp.logical_not(left))
        def _():
            relay_right(k, low, high, across)

    def over_in(k):
        @pl.when(left)
        def _():
            over_right(k)

        @pl.when(jnp.logical_not(left))
        def _():
            over_left(k)

    def over_out(k):
        @pl.when(left)
        def _():
            over_left(k)

        @pl.when(jnp.logical_not(left))
        def _():
            over_right(k)

    for load in loads[2:6]:
        load.wait()
    gains = jnp.broadcast_to(gain[...], (8, R)).T[:, 0:1]

    def rows_of(n):
        return pl.ds(pl.multiple_of(n * step, step), step)

    def send_gu(i):
        e = send_order(i)
        gu_send[e, :, :C] = (eg[e] * gains).astype(BF)
        gu_send[e, :, C:] = (eu[e] * gains).astype(BF)

        @pl.when(e != g)
        def _():
            def piece(n):
                remote(
                    gu_send.at[e, rows_of(n)],
                    gu.at[f, rows_of(n)],
                    s_gu.at[0],
                    r_gu.at[g, n],
                    2 * e + p,
                    t,
                ).start()

            loop(0, pieces, piece)

    loop(0, D, send_gu)
    gu[f] = gu_send[g]

    for load in loads[6:]:
        load.wait()
    sh[f, 0] = sd[...].T.astype(BF)
    sh[f, 1] = (sg[...] * gains).astype(BF)
    sh[f, 2] = (su[...] * gains).astype(BF)
    spread(f)
    at_end = (g == 0) | (g == G - 1)

    @pl.when(at_end)
    def _():
        loop(0, 3, lambda i: share_left(f, i))
        loop(0, 3, lambda i: share_right(f, i))

    loop(D, E, send_gu)

    def cross(src, n):
        remote(
            gu.at[src, rows_of(n)],
            gu.at[src, rows_of(n)],
            f_gu.at[0],
            x_gu.at[0],
            pair,
            t,
        ).start()

    loop(0, pieces, lambda n: cross(f, n))

    loop(0, 3, lambda i: share_pair(f, i))

    def take_block(group):
        arrived(port.at[t, group], s_load.at[0], r_port.at[0, group])
        pass_block(group)

    def take_side(i):
        @pl.when(i != depth)
        def _():
            take_block(at_depth(i))

    def take_other(i):
        take_block(at_depth(G - 1 - i))

    def open_block(i):
        group = at_depth(G - 1 - i)
        arrived(raw.at[i], s_load.at[0], r_raw.at[i])
        arrived(meta.at[i], s_load.at[0], r_meta.at[i])
        for k in range(D - 1):
            gw_send[i, k] = pack(at_depth(k), meta[i], raw[i])
            remote(
                gw_send.at[i, k],
                port.at[t, group],
                s_gw.at[0],
                r_port.at[0, group],
                2 * at_depth(k) + p,
                t,
            ).start()
        port[t, group] = pack(g, meta[i], raw[i])
        pass_block(group)

    def inner_block(i):
        group = near_first(i)
        for o in range(1, H):
            src = (t + 2 * o) % T
            arrived(port.at[src, group], s_load.at[0], r_port.at[o, group])
            port_copy(src, group, p_in.at[0], x_port.at[0], t_pair).start()


    def take_near(i):
        src = 2 * jnp.where(2 * g < G, i, G - 1 - i) + p

        @pl.when(src != f)
        def _():
            def piece(n):
                arrived(gu.at[src, rows_of(n)], s_load.at[0], r_gu.at[src // 2, n])
                cross(src, n)

            loop(0, pieces, piece)


    def take_far(n):
        def block(i):
            src = 2 * jnp.where(2 * g < G, G // 2 + i, G // 2 - 1 - i) + p
            arrived(gu.at[src, rows_of(n)], s_load.at[0], r_gu.at[src // 2, n])
            cross(src, n)

        loop(0, G // 2, block)


    def expert_hidden(i):
        group = near_first(i)
        total = jnp.zeros((slots, 2 * C), F32)
        squares = jnp.zeros((slots, 1), F32)
        for q in range(T):
            total = total + dot(
                port[q, group], gu[q * K : (q + 1) * K].reshape(quarter, 2 * C)
            )
            x = port[q, group].astype(F32)
            squares = squares + jnp.sum(x * x, axis=1, keepdims=True)
        total = total * lax.rsqrt(squares / width + EPS)
        hid[t, group] = (silu(total[:, :C]) * total[:, C:]).astype(BF)
        for o in range(1, H):
            remote(
                hid.at[t, group],
                hid.at[t, group],
                s_out.at[0],
                r_hid.at[H - o, group],
                f,
                (t + 2 * o) % T,
            ).start()
        remote(
            hid.at[t, group],
            hid.at[t, group],
            s_in.at[0],
            r_hid.at[0, group],
            f,
            t_pair,
        ).start()


    def pass_hidden(i):
        group = near_first(i)
        for o in range(1, H):
            src = (t + 2 * o) % T
            arrived(hid.at[src, group], s_load.at[0], r_hid.at[o, group])
            remote(
                hid.at[src, group],
                hid.at[src, group],
                s_in.at[0],
                r_hid.at[0, group],
                f,
                t_pair,
            ).start()


    def send_ret(group):
        remote(
            ret_send.at[group], ret.at[g], s_ret.at[0], r_ret.at[0], 2 * group + p, t
        ).start()

    def expert_out(i):
        group = near_first(i)
        arrived(hid.at[:H, group], s_load.at[0], r_hid.at[0, group])
        total = jnp.zeros((slots, quarter), F32)
        for q in range(T):
            total = total + dot_nt(hid[q, group], dn[:, q].reshape(K * R, C))
        ret_send[group] = total.astype(BF)

        @pl.when((group != g) & (i < G - 1))
        def _():
            send_ret(group)


    at_gate = depth == D - 1

    @pl.when(at_gate)
    def _():
        loop(0, D, lambda i: open_block(D - 1 - i))

    loop(0, D, take_side)

    def send_dn(i):
        e = send_order(i)
        dn_send[e] = ed[e].astype(BF)

        @pl.when(jnp.logical_not((e == g) & mine))
        def _():
            remote(
                dn_send.at[e], dn.at[f % K, t], s_dn.at[0], r_dn.at[f % K // 2, t], 2 * e + p, home
            ).start()

    loop(0, E, send_dn)

    @pl.when(mine)
    def _():
        dn[f % K, t] = dn_send[g]

    @pl.when(jnp.logical_not(at_end))
    def _():
        loop(0, 3, lambda i: share_left(f, i))
        loop(0, 3, lambda i: share_right(f, i))


    def hand_across(i):
        k = 2 * i + p

        def chunk(q):
            @pl.when(jnp.logical_not((t * K + k == f) & (q == t)))
            def _():
                arrived(dn.at[k, q], s_load.at[0], r_dn.at[i, q])

            remote(dn.at[k, q], dn.at[k, q], f_dn.at[0], x_dn.at[0], pair, t).start()

        loop(0, T, chunk)

    loop(0, G // 2, take_near)
    loop(1, G // 2, relay_in)
    loop(1, G // 2, over_in)
    loop(0, pieces // 2, take_far)

    @pl.when(jnp.logical_not(at_gate))
    def _():
        loop(0, D, lambda i: take_other(D - 1 - i))

    loop(pieces // 2, pieces, take_far)
    @pl.when(at_end)
    def _():
        loop(0, K // 2, hand_across)

    loop(0, G, inner_block)
    @pl.when(jnp.logical_not(at_end))
    def _():
        loop(0, K // 2, hand_across)


    for o in range(1, H):
        src = (t + 2 * o) % T
        arrived(tk.at[src], s_load.at[0], r_tok.at[src])
        tok_copy(src, s_tok.at[0], t_pair).start()
    for o in range(H):
        src = (t_pair + 2 * o) % T
        arrived(tk.at[src], s_load.at[0], r_tok.at[src])
    squares = jnp.zeros((tok_count, 1), F32)
    for q in range(T):
        x = tk[q].astype(F32)
        squares = squares + jnp.sum(x * x, axis=1, keepdims=True)
    scale = lax.rsqrt(squares / width + EPS)
    for q in range(T):
        nm[q] = (tk[q].astype(F32) * scale).astype(BF)
    arrived(port.at[:H], s_load.at[0], x_port.at[0])
    arrived(gu.at[:G], s_load.at[0], x_gu.at[0])
    loop(0, G, expert_hidden)
    loop(1, min(2, G), lambda k: relay_out(k, across=True))
    loop(0, G, pass_hidden)
    @pl.when(jnp.logical_not(at_end))
    def _():
        loop(2, G // 2 + 1, relay_out)
        loop(2, G // 2 + 1, over_out)

    @pl.when(at_end)
    def _():
        loop(2, G // 2 + 1, lambda k: relay_out(k, across=True))

    arrived(dn.at[: K // 2], s_load.at[0], x_dn.at[0])
    loop(0, G, expert_out)
    ret[g] = ret_send[g]


    def late_out(k):
        relay_out(k, across=True)

    def late_in(k):
        relay_in(k, across=True)

    loop(G // 2 + 1, G, late_out)
    loop(G // 2, G, late_in)

    def place_down(k):
        for q in range(0, T, 2):
            a, b = dn[k, q].astype(F32), dn[k, q + 1].astype(F32)
            block = jnp.where(
                p == 0, left_halves(a, b, half), right_halves(a, b, half)
            )
            dn_out[pl.ds(pl.multiple_of(k * R, R), R), q * half : (q + 2) * half] = block.astype(BF)

    loop(0, K, place_down)

    def wait_down(i):
        block = near_first(i) * 2 + 1 - p
        arrived(sh.at[block, 0], s_load.at[0], r_shp.at[block // 2, 0])
        spread(block)
        arrived(sh.at[block, 1:3], s_load.at[0], r_shp.at[block // 2, 1])

    send_ret(near_first(G - 1))
    loop(0, G, wait_down)

    gate_sh = sh[:, 1].reshape(F * R, C)
    up_sh = sh[:, 2].reshape(F * R, C)
    act = jnp.zeros((tok_count, C), F32)
    lin = jnp.zeros((tok_count, C), F32)
    for q in range(T):
        act = act + dot(nm[q], gate_sh[q * quarter : (q + 1) * quarter])
        lin = lin + dot(nm[q], up_sh[q * quarter : (q + 1) * quarter])
    hsh[t] = (silu(act) * lin).astype(BF)

    def send_hsh(d):
        remote(
            hsh.at[t], hsh.at[t], s_hsh.at[0], r_hsh.at[0], f, (t + d) % T
        ).start()

    loop(1, T, send_hsh)

    def keep_down(k):
        sdx[t, k] = sh[t * K + k, 0]

    loop(0, K, keep_down)

    for q in range(T):
        span = slice(q * quarter, (q + 1) * quarter)
        sd_out[:, span] = (
            sh[q * K : (q + 1) * K, 0].reshape(quarter, C).astype(F32).T.astype(BF)
        )
    sg_out[...] = sh[:, 1].reshape(F * R, C)
    su_out[...] = sh[:, 2].reshape(F * R, C)

    for q in range(T):
        span = slice(q * quarter, (q + 1) * quarter)
        whole = gu[q * K : (q + 1) * K].reshape(quarter, 2 * C).astype(F32)
        gate, up = whole[:, :C].T, whole[:, C:].T
        gate_out[:, span] = jnp.where(p == 0, gate[:half], gate[half:]).astype(BF)
        up_out[:, span] = jnp.where(p == 0, up[:half], up[half:]).astype(BF)

    experts = lax.broadcasted_iota(jnp.int32, (tok_count, E), 1)
    turned = jnp.where(line == 2, weight[0:1, :], meta_send[...])
    turned = jnp.where(line == 3, weight[1:2, :], turned).T
    first, second = turned[:, 0:1].astype(jnp.int32), turned[:, 1:2].astype(jnp.int32)
    named = ((experts == first) | (experts == second)).astype(F32)
    before = (cols < rows).astype(F32).astype(BF)
    place = dot(before, named.astype(BF))
    slot_ids = lax.broadcasted_iota(jnp.int32, (tok_count, E * slots), 1)

    def pick_of(chosen):
        spot = jnp.sum(jnp.where(experts == chosen, place, 0.0), axis=1, keepdims=True)
        return slot_ids == chosen * slots + spot.astype(jnp.int32)

    pick0, pick1 = pick_of(first), pick_of(second)

    arrived(ret.at[: G - 1], s_load.at[0], r_ret.at[0])
    outs = ret[...].reshape(E * slots, quarter)
    routed = jnp.zeros((tok_count, quarter), F32)
    for k, pick in enumerate((pick0, pick1)):
        chosen = jnp.where(pick, 1.0, 0.0).astype(BF)
        routed = routed + turned[:, 2 + k : 3 + k] * dot(chosen, outs)

    arrived(sdx.at[: T - 1], s_load.at[0], r_sdx.at[0])
    arrived(hsh.at[: T - 1], s_load.at[0], r_hsh.at[0])
    for q in range(T):
        routed = routed + dot_nt(hsh[q], sdx[q].reshape(K * R, C))
    mixed[...] = routed.astype(BF)

    def gone(ref, sem):
        sent(ref, sem.at[0], sem.at[0])

    gone(tk.at[: T - 1], s_tok)
    gone(hsh.at[: T - 1], s_hsh)
    gone(tok, s_raw)
    gone(meta_send, s_meta)
    gone(gu.at[:G], f_gu)
    gone(gu.at[: E - 1], s_gu)
    gone(dn.at[: K // 2], f_dn)
    gone(ret.at[: G - 1], s_ret)
    gone(port.at[:H], p_in)
    gone(hid.at[:H], s_in)
    gone(sh.at[:G], s_shb)
    gone(sdx.at[: T - 1], s_sdx)
    if H > 1:
        gone(port.at[: H - 1], p_out)
        gone(hid.at[: H - 1], s_out)
    if D > 1:
        gone(disp.at[: D - 1], s_da)

        @pl.when(at_gate)
        def _():
            gone(gw_send, s_gw)

    @pl.when(mine)
    def _():
        gone(dn_send.at[: E - 1], s_dn)

    @pl.when(jnp.logical_not(mine))
    def _():
        gone(dn_send, s_dn)

    def done_groups(d):
        @pl.when((d >= g) & (g > 0))
        def _():
            sent(sh.at[f], s_left.at[d], s_left.at[d])

        @pl.when((d <= g) & (g < G - 1))
        def _():
            sent(sh.at[f], s_right.at[d], s_right.at[d])

    loop(0, G, done_groups)


def hand_on(count, *refs):
    copies = [
        pltpu.make_async_copy(refs[i], refs[count + i], refs[-1].at[i])
        for i in range(count)
    ]
    for copy in copies:
        copy.start()
    for copy in copies:
        copy.wait()


def on_device(
    tokens,
    routes,
    route_weight,
    norm_gain,
    expert_gate,
    expert_up,
    expert_down,
    shared_gate,
    shared_up,
    shared_down,
):
    F = lax.axis_size("fs")
    T = lax.axis_size("tp")
    E, R, C = expert_gate.shape
    tok_count, quarter = tokens.shape
    pick_count = routes.shape[1]
    capacity = 2 * ((3 * tok_count * pick_count + 4 * E - 1) // (4 * E))
    slots = (capacity + 15) // 16 * 16
    G, K = F // 2, F // T
    vmem = pl.BlockSpec(memory_space=pltpu.VMEM)
    hbm = pl.BlockSpec(memory_space=pltpu.HBM)
    dma = pltpu.SemaphoreType.DMA
    shapes = [
        (tok_count, quarter),
        (C // 2, F * R),
        (C // 2, F * R),
        (K * R, T * C // 2),
        (F * R, C),
        (F * R, C),
        (C, F * R),
    ]
    H, D, N = T // 2, G // 2, max(R // 128, 1)
    scratch = [
        (T, tok_count, quarter),
        (T, tok_count, quarter),
        (E, R, 2 * C),
        (F, R, 2 * C),
        (E, R, C),
        (K, T, R, C),
        (F, 3, R, C),
        (D, slots, quarter),
        (T, G, slots, quarter),
        (T, G, slots, C),
        (G, slots, quarter),
        (G, slots, quarter),
        (T, tok_count, C),
        (T, K, R, C),
        (D, tok_count, quarter),
        (D, max(D - 1, 1), slots, quarter),
    ]
    wide = [(8, tok_count), (D, 8, tok_count)]
    one = (1,)
    sems = [
        one, (T,), one, (G, N), one, one, one, (K // 2, T), one, one,
        (G,), (G,), one, (G, 3), (G, 2), one, one, one, (H, G), one,
        one, (D,), one, (D,), one, one, one, (H, G), one, one, one, one, one, one,
    ]
    args = (
        tokens,
        routes.T,
        route_weight.T,
        norm_gain[None, :],
        expert_gate,
        expert_up,
        expert_down,
        shared_gate,
        shared_up,
        shared_down,
    )
    results = pl.pallas_call(
        functools.partial(kernel, F, T, slots),
        out_shape=[jax.ShapeDtypeStruct(s, BF) for s in shapes],
        in_specs=[hbm] * 10,
        out_specs=[vmem] * 7,
        scratch_shapes=[pltpu.VMEM(a.shape, a.dtype) for a in args]
        + [dma((len(args),))]
        + [pltpu.VMEM(s, BF) for s in scratch]
        + [pltpu.VMEM(s, F32) for s in wide]
        + [dma(s) for s in sems],
        compiler_params=pltpu.CompilerParams(
            has_side_effects=True, collective_id=0, vmem_limit_bytes=48 * 1024 * 1024
        ),
    )(*[pltpu.with_memory_space_constraint(a, pltpu.HBM) for a in args])
    mixed, gate, up, down, sg, su, sd = pl.pallas_call(
        functools.partial(hand_on, 7),
        out_shape=[jax.ShapeDtypeStruct(s, BF) for s in shapes],
        in_specs=[vmem] * 7,
        out_specs=[hbm] * 7,
        scratch_shapes=[dma((7,))],
        compiler_params=pltpu.CompilerParams(vmem_limit_bytes=8 * 1024 * 1024),
    )(*results)
    return (mixed, gate.T[None], up.T[None], down[None], sg, su, sd)


def solution(mesh):
    in_specs = (
        P("fs", "tp"),
        P("fs", None),
        P("fs", None),
        P("fs"),
        P(None, "fs", "tp"),
        P(None, "fs", "tp"),
        P(None, "fs", "tp"),
        P("fs", "tp"),
        P("fs", "tp"),
        P("tp", "fs"),
    )
    out_specs = (
        P("fs", "tp"),
        P("fs", None, "tp"),
        P("fs", None, "tp"),
        P("fs", "tp", None),
        P(None, "tp"),
        P(None, "tp"),
        P("tp", None),
    )
    return jax.shard_map(
        on_device, mesh=mesh, in_specs=in_specs, out_specs=out_specs, check_vma=False
    )
```
